32 devices in a mesh: ep: 16 (over z, y, x), tp: 2 (over core).
Axes of the slice: x: 2, y: 2, z: 4, core: 2. Of those that a mesh axis runs over, the one named last changes fastest.
Arguments:
- residual: bfloat16 [256, 2048], P(('ep', 'tp')), may hold values from -6 to 6
- query_latent: bfloat16 [256, 8, 512], P(('ep', 'tp')), may hold values from -40 to 40
- query_rotary: bfloat16 [256, 8, 32], P(('ep', 'tp')), may hold values from -6 to 6
- latent_new: bfloat16 [256, 512], P(('ep', 'tp')), may hold values from -16 to 16
- rotary_new: bfloat16 [256, 32], P(('ep', 'tp')), may hold values from -6 to 6
- latent_cache: bfloat16 [256, 256, 512], P(('ep', 'tp')), may hold values from -16 to 16
- rotary_cache: bfloat16 [256, 256, 32], P(('ep', 'tp')), may hold values from -6 to 6
- lengths: int32 [256], P(('ep', 'tp')), may hold values from 32 to 256, as said below
- value_up: bfloat16 [512, 8, 64], replicated, may hold values from -1 to 1
- out_proj: bfloat16 [512, 2048], replicated, may hold values from -0.5 to 0.5
- attn_gain: bfloat16 [2048], replicated, may hold values from 0.099609375 to 1.8984375
- mix_gate: bfloat16 [2048], replicated, may hold values from -0.125 to 0.125
- dense_w_gate: bfloat16 [2048, 2048], P(None, 'ep'), may hold values from -0.125 to 0.125
- dense_w_up: bfloat16 [2048, 2048], P(None, 'ep'), may hold values from -0.125 to 0.125
- dense_w_down: bfloat16 [2048, 2048], P('ep'), may hold values from -0.5 to 0.5
- expert_ids: int32 [256, 6], P(('ep', 'tp')), may hold values from 0 to 15, all different within a row; in each aligned block of 16 rows (0 to 15, 16 to 31, ...) at most 12 rows name the same one
- expert_scores: float32 [256, 6], P(('ep', 'tp')), may hold values from 0.1 to 5
- expert_gate: bfloat16 [16, 2048, 512], P('ep', None, 'tp'), may hold values from -0.125 to 0.125
- expert_up: bfloat16 [16, 2048, 512], P('ep', None, 'tp'), may hold values from -0.125 to 0.125
- expert_down: bfloat16 [16, 512, 2048], P('ep', 'tp'), may hold values from -1 to 1
- out_gain: bfloat16 [2048], replicated, may hold values from 0.099609375 to 1.8984375
Outputs:
- layer_out: bfloat16 [256, 2048], P(('ep', 'tp'))
The draws below stay inside these ranges and needn't reach their ends.
Inputs may be any that keep to these rules, and one draw needn't show every extreme that they name: `expert_ids`: within each aligned block of 16 rows (the sequences of one ep index) no expert is named by more than 12 rows, a bound that some block reaches; a row names 6 different experts. `lengths`: some sequence has exactly 256 cached positions.
All inputs are finite; a program needn't handle non-finite values.
Results may differ from the reference program's by a relative error of at most 0.018.
Values may be sent and summed in bfloat16 or wider, within the bound.
A program may use at most 128 MiB of HBM per device.

```python
import math
import jax
import jax.numpy as jnp
import numpy as np
from jax import lax

D = 2048
H = 8
KL = 512
ROPE = 32
NOPE = 64
V = 64
FE = 512
FD = 2048
TOPK = 6
SEQ_DEV = 8
CACHE = 256
EXPERTS = 16
TOK_GROUP = 16
SEQS = 256
CAP = 12
N_TP = 2


def draw_latent_cache(key, part):
    values = jnp.clip(jax.random.normal(jax.random.fold_in(key, 1), (SEQS, CACHE, KL), jnp.float32), -6.0, 6.0)
    return values.astype(jnp.bfloat16)


def draw_query_latent(key, part):
    values = 0.5 * jnp.clip(jax.random.normal(jax.random.fold_in(key, 2), (SEQS, H, KL), jnp.float32), -6.0, 6.0)
    return values.astype(jnp.bfloat16)


def draw_lengths(key, part):
    keys = jax.random.split(jax.random.fold_in(key, 3), 3)
    short = jax.random.randint(keys[0], (SEQS,), CACHE // 8, CACHE + 1)
    full = jax.random.randint(keys[1], (SEQS,), 0, 4) == 0
    values = jnp.where(full, CACHE, short)
    values = values.at[jax.random.randint(keys[2], (), 0, SEQS)].set(CACHE)
    return values.astype(jnp.int32)


def steps_of(own_key, dims, shards, low, top_value):
    level, own = 1.0, jax.random.fold_in(own_key, 6)
    for dim, shards_of in shards:
        steps = jnp.exp(jax.random.uniform(jax.random.fold_in(own, dim), (shards_of,), jnp.float32, low / len(shards), top_value / len(shards)))
        level = level * jnp.repeat(steps, dims[dim] // shards_of).reshape([-1 if axis == dim else 1 for axis in range(len(dims))])
    return level


def routed_block(stream_key, own, number, rows, count, top, bound, slope):
    ranking = jax.random.permutation(stream_key, count)
    crowded, common = portions_of(count, rows * top, bound, slope, True), portions_of(count, rows * top, bound, slope, False)
    places = jnp.arange(count)

    def named(tallies, rotation):
        used = int((tallies > 0).sum())
        fixed = max(1, used // 4)
        shifted = fixed + (places - fixed + rotation * (used - fixed)) % max(1, count - fixed)
        return jnp.zeros((count,), jnp.int32).at[ranking[jnp.where(places < fixed, places, shifted)]].set(jnp.asarray(tallies, jnp.int32))

    tallies = jnp.where(number % 4 == 0, named(crowded, number // 4), named(common, number - number // 4 - 1))
    mixed = jax.random.permutation(jax.random.fold_in(own, 3), count)
    giver, sink = mixed[0:count // 2 * 2:2], mixed[1:count // 2 * 2:2]
    room = jnp.minimum(tallies[giver] - 1, bound - tallies[sink]) // 2
    room = jnp.where((giver == ranking[0]) | (sink == ranking[0]) | (tallies[sink] == 0), 0, jnp.maximum(room, 0))
    shifted = jax.random.randint(jax.random.fold_in(own, 4), (count // 2,), 0, 1 << 20) % (room + 1)
    tallies = tallies.at[giver].add(-shifted).at[sink].add(shifted)
    labels = jnp.searchsorted(jnp.cumsum(tallies), jnp.arange(rows * top), side="right").astype(jnp.int32)
    table = labels.reshape(top, rows).T
    table = table[jax.random.permutation(jax.random.fold_in(own, 1), rows)]
    rotation = jax.random.randint(jax.random.fold_in(own, 2), (rows, 1), 0, top)
    return jnp.take_along_axis(table, (jnp.arange(top)[None, :] + rotation) % top, axis=1)


def portions_of(amount, total, limit, lean, full):
    portions = [(1 << 20) // math.isqrt(rank ** lean) + 1 for rank in range(1, amount + 1)]
    largest = limit if full else min(limit, max(-(-total // amount), total * portions[0] // sum(portions)))
    least = 1 if total - largest >= amount - 1 else 0
    holding, spare = [largest] + [least] * (amount - 1), total - largest - least * (amount - 1)
    while spare > 0:
        free = [i for i in range(1, amount) if holding[i] < largest] or [i for i in range(1, amount) if holding[i] < limit]
        pool, left = sum([portions[i] for i in free]), spare
        for i in free:
            extra = min(limit - holding[i], max(1, left * portions[i] // pool), spare)
            holding[i] = holding[i] + extra
            spare = spare - extra
    return np.array(holding)


def normal_values(own_key, dims, deviation, bound, cuts=(), kind=jnp.bfloat16):
    level = steps_of(own_key, dims, cuts, -0.22, 0.18) if cuts else 1.0
    values = jax.random.normal(own_key, dims, jnp.float32) * deviation * level
    return jnp.minimum(jnp.maximum(values, -bound), bound).astype(kind)


def setup_inputs(seed: int = 0) -> dict:
    splits = jax.random.split(jax.random.key(seed), 22)
    residual = normal_values(splits[0], (SEQS, D), 1.0, 6.0, ((0, 32),))
    query_latent = draw_query_latent(jax.random.fold_in(splits[21], 71), 0)
    query_rotary = normal_values(splits[2], (SEQS, H, ROPE), 1.0, 6.0, ((0, 32),))
    latent_new = normal_values(splits[3], (SEQS, KL), 3.0, 16.0, ((0, 32),))
    rotary_new = normal_values(splits[4], (SEQS, ROPE), 1.0, 6.0, ((0, 32),))
    latent_cache = draw_latent_cache(jax.random.fold_in(splits[21], 71), 0)
    rotary_cache = normal_values(splits[6], (SEQS, CACHE, ROPE), 1.0, 6.0, ((0, 32),))
    lengths = draw_lengths(jax.random.fold_in(splits[21], 71), 0)
    value_up = normal_values(splits[8], (KL, H, V), (KL // 16) ** -0.5, 1.0)
    out_proj = normal_values(splits[9], (H * V, D), (H * V // 4) ** -0.5, 0.5)
    attn_gain = jnp.clip(1.0 + 0.18 * jax.random.normal(splits[10], (D,), jnp.float32), 0.099609375, 1.8984375).astype(jnp.bfloat16)
    mix_gate = normal_values(splits[11], (D,), D ** -0.5, 0.125)
    dense_w_gate = normal_values(splits[12], (D, FD), D ** -0.5, 0.125, ((1, 16),))
    dense_w_up = normal_values(splits[13], (D, FD), D ** -0.5, 0.125, ((1, 16),))
    dense_w_down = normal_values(splits[14], (FD, D), (FD // 16) ** -0.5, 0.5, ((0, 16),))
    expert_ids_keys = jax.random.split(jax.random.fold_in(splits[15], 1), SEQS // TOK_GROUP)
    expert_ids_turns = jax.random.permutation(jax.random.fold_in(splits[15], 3), SEQS // TOK_GROUP)
    expert_ids = jax.vmap(lambda own, number: routed_block(jax.random.fold_in(splits[15], 2), own, number, TOK_GROUP, EXPERTS, TOPK, CAP, 2))(expert_ids_keys, expert_ids_turns).reshape((SEQS, TOPK))
    expert_scores = jnp.clip(jnp.exp(math.log(5.0) - 3.912023 * jax.random.uniform(splits[16], (SEQS, TOPK), jnp.float32) ** steps_of(splits[16], (SEQS, TOPK), ((0, 32),), -0.2, 0.2)), 0.1, 5.0)
    expert_gate = normal_values(splits[17], (EXPERTS, D, FE), D ** -0.5, 0.125, ((0, 16), (2, 2)))
    expert_up = normal_values(splits[18], (EXPERTS, D, FE), D ** -0.5, 0.125, ((0, 16), (2, 2)))
    expert_down = normal_values(splits[19], (EXPERTS, FE, D), (FE // 16) ** -0.5, 1.0, ((0, 16), (1, 2)))
    out_gain = jnp.clip(1.0 + 0.18 * jax.random.normal(splits[20], (D,), jnp.float32), 0.099609375, 1.8984375).astype(jnp.bfloat16)
    return dict(residual=residual, query_latent=query_latent, query_rotary=query_rotary, latent_new=latent_new, rotary_new=rotary_new, latent_cache=latent_cache, rotary_cache=rotary_cache, lengths=lengths, value_up=value_up, out_proj=out_proj, attn_gain=attn_gain, mix_gate=mix_gate, dense_w_gate=dense_w_gate, dense_w_up=dense_w_up, dense_w_down=dense_w_down, expert_ids=expert_ids, expert_scores=expert_scores, expert_gate=expert_gate, expert_up=expert_up, expert_down=expert_down, out_gain=out_gain)


ALPHA = 8.0 ** 0.25
EPS = 1e-06
ROPE_BASE = 10000.0

def rotate(vector, position):
    half_dim = vector.shape[-1] // 2
    inv_freq = ROPE_BASE ** (-jnp.arange(half_dim, dtype=jnp.float32) / half_dim)
    angles = position.astype(jnp.float32)[..., None] * inv_freq
    cosine = jnp.cos(angles)
    sine_part = jnp.sin(angles)
    lower_half = vector[..., :half_dim]
    upper_half = vector[..., half_dim:]
    return jnp.concatenate([lower_half * cosine - upper_half * sine_part, upper_half * cosine + lower_half * sine_part], axis=-1)

def normalize(values, gain):
    center = lax.optimization_barrier(jnp.mean(values, -1, keepdims=True))
    spread = lax.optimization_barrier(jnp.mean(jnp.square(values - center), -1, keepdims=True))
    return (values - center) * lax.rsqrt(spread + EPS) * gain.astype(jnp.float32)

def attend(block):
    query_latent, query_rotary, latent_new, rotary_new, latent_cache, rotary_cache, lengths = block
    score_scale = (NOPE + ROPE) ** (-0.5)
    query_turned = rotate(query_rotary.astype(jnp.float32), lengths[:, None]).astype(jnp.bfloat16)
    key_turned = rotate(rotary_new.astype(jnp.float32), lengths).astype(jnp.bfloat16)
    query_wide = query_latent.astype(jnp.float32)
    turned_wide = query_turned.astype(jnp.float32)
    cache_wide = latent_cache.astype(jnp.float32)
    new_wide = latent_new.astype(jnp.float32)
    scores = (jnp.einsum('bhr,btr->bht', query_wide, cache_wide) + jnp.einsum('bhe,bte->bht', turned_wide, rotary_cache.astype(jnp.float32))) * score_scale
    own_score = (jnp.einsum('bhr,br->bh', query_wide, new_wide) + jnp.einsum('bhe,be->bh', turned_wide, key_turned.astype(jnp.float32))) * score_scale
    live = jnp.arange(CACHE, dtype=jnp.int32)[None, :] < lengths[:, None]
    scores = jnp.where(live[:, None, :], scores, -jnp.inf)
    top_score = jnp.maximum(lax.optimization_barrier(jnp.max(scores, -1)), own_score)
    cache_probs = jnp.exp(scores - top_score[..., None])
    own_prob = jnp.exp(own_score - top_score)
    prob_total = lax.optimization_barrier(jnp.sum(cache_probs, -1)) + own_prob
    cache_weights = (cache_probs / prob_total[..., None]).astype(jnp.bfloat16)
    own_weight = (own_prob / prob_total).astype(jnp.bfloat16)
    latent_out = jnp.einsum('bht,btr->bhr', cache_weights.astype(jnp.float32), cache_wide) + own_weight.astype(jnp.float32)[..., None] * new_wide[:, None, :]
    return latent_out.astype(jnp.bfloat16)

def expert_block(block):
    token_rows, gate_weight, up_weight, down_weight = block
    flat_rows = token_rows.reshape(-1, D)
    half_width = FE // N_TP
    summed = jnp.zeros(flat_rows.shape, jnp.float32)
    for part_index in range(N_TP):
        lower = part_index * half_width
        upper = lower + half_width
        gate_pre = jnp.dot(flat_rows, gate_weight[:, lower:upper], preferred_element_type=jnp.float32)
        up_pre = jnp.dot(flat_rows, up_weight[:, lower:upper], preferred_element_type=jnp.float32)
        hidden_part = (jax.nn.silu(gate_pre) * up_pre).astype(jnp.bfloat16)
        part_out = jnp.dot(hidden_part, down_weight[lower:upper], preferred_element_type=jnp.float32).astype(jnp.bfloat16)
        summed = summed + part_out.astype(jnp.float32)
    return summed.astype(jnp.bfloat16).reshape(token_rows.shape)

def reference(residual, query_latent, query_rotary, latent_new, rotary_new, latent_cache, rotary_cache, lengths, value_up, out_proj, attn_gain, mix_gate, dense_w_gate, dense_w_up, dense_w_down, expert_ids, expert_scores, expert_gate, expert_up, expert_down, out_gain):
    block_count = SEQS // SEQ_DEV

    def split_blocks(array):
        return array.reshape((block_count, SEQ_DEV) + array.shape[1:])
    latent_out = lax.map(attend, (split_blocks(query_latent), split_blocks(query_rotary), split_blocks(latent_new), split_blocks(rotary_new), split_blocks(latent_cache), split_blocks(rotary_cache), split_blocks(lengths)))
    latent_out = latent_out.reshape(SEQS, H, KL)
    heads_out = jnp.einsum('bhr,rhv->bhv', latent_out.astype(jnp.float32), value_up.astype(jnp.float32))
    heads_out = heads_out.astype(jnp.bfloat16).reshape(SEQS, H * V)
    attn = jnp.dot(heads_out, out_proj, preferred_element_type=jnp.float32).astype(jnp.bfloat16)
    mixed = normalize(ALPHA * residual.astype(jnp.float32) + attn.astype(jnp.float32), attn_gain).astype(jnp.bfloat16)
    mix = jax.nn.sigmoid(jnp.dot(mixed, mix_gate, preferred_element_type=jnp.float32))
    gate_pre = jnp.dot(mixed, dense_w_gate, preferred_element_type=jnp.float32)
    up_pre = jnp.dot(mixed, dense_w_up, preferred_element_type=jnp.float32)
    hidden = (jax.nn.silu(gate_pre) * up_pre).astype(jnp.bfloat16)
    dense_out = jnp.dot(hidden, dense_w_down, preferred_element_type=jnp.float32).astype(jnp.bfloat16)
    group_count = SEQS // TOK_GROUP
    route_ids = expert_ids.reshape(group_count, TOK_GROUP * TOPK)
    onehot = (route_ids[..., None] == jnp.arange(EXPERTS, dtype=jnp.int32)).astype(jnp.int32)
    slot_index = lax.optimization_barrier(jnp.sum((jnp.cumsum(onehot, 1) - 1) * onehot, -1)).astype(jnp.int32)
    group_index = jnp.broadcast_to(jnp.arange(group_count, dtype=jnp.int32)[:, None], route_ids.shape)
    token_rows = jnp.repeat(mixed.reshape(group_count, TOK_GROUP, D), TOPK, axis=1)
    buffer = jnp.zeros((EXPERTS, group_count, CAP, D), jnp.bfloat16).at[route_ids, group_index, slot_index].set(token_rows)
    expert_out = lax.map(expert_block, (buffer, expert_gate, expert_up, expert_down))
    picked = expert_out[route_ids, group_index, slot_index].reshape(SEQS, TOPK, D)
    share = expert_scores / lax.optimization_barrier(jnp.sum(expert_scores, 1, keepdims=True))
    routed = lax.optimization_barrier(jnp.sum(picked.astype(jnp.float32) * share[:, :, None], 1))
    summed_total = ALPHA * mixed.astype(jnp.float32) + routed + mix[:, None] * dense_out.astype(jnp.float32)
    return normalize(summed_total, out_gain).astype(jnp.bfloat16)
```

```python
import functools
import math

import jax
import jax.numpy as jnp
from jax import lax
from jax.experimental import pallas as pl
from jax.experimental.pallas import tpu as pltpu
from jax.sharding import PartitionSpec as P

NOPE = 64
ALPHA = 8.0**0.25
EPS = 1e-06
ROPE_BASE = 10000.0
F32 = jnp.float32
BF16 = jnp.bfloat16
MESH = pl.DeviceIdType.MESH
VMEM = pltpu.VMEM


def inner_size(n):
    size = 1
    while size * size < n:
        size *= 2
    return size if n % size == 0 else n


def silu(value):
    return value / (1.0 + jnp.exp(-value))


def dot(a, b):
    return jnp.dot(a, b, preferred_element_type=F32)


def dot_nt(a, b):
    return lax.dot_general(a, b, (((1,), (1,)), ((), ())), preferred_element_type=F32)


def row_sum(value):
    return jnp.sum(value, -1, keepdims=True)


def kernel(
    n,
    group,
    lengths,
    qr_hbm,
    rn_hbm,
    ql_hbm,
    ln_hbm,
    rc_hbm,
    cache_hbm,
    res_hbm,
    ids_hbm,
    rs_hbm,
    vu_hbm,
    op_hbm,
    ag_hbm,
    mg_hbm,
    eg_hbm,
    eu_hbm,
    ed_hbm,
    dg_hbm,
    du_hbm,
    dd_hbm,
    og_hbm,
    out,
    query_rotary,
    rotary_new,
    query_latent,
    latent_new,
    rotary_cache,
    cache,
    ids,
    route_scores,
    vu,
    op,
    attn_gain,
    mix_gate,
    eg,
    eu,
    down,
    dg,
    du,
    out_gain,
    lat,
    rows_all,
    heads_all,
    wide_rows,
    mixed,
    scale,
    hid,
    sbuf,
    rbuf,
    zbuf,
    zrecv,
    in_sem,
    cache_sem,
    w_send,
    w_recv,
    r_send,
    r_line,
    r_plane,
    h_send,
    h_recv,
    s_send,
    s_plane,
    s_line,
):
    me = lax.axis_index("ep")
    core = lax.axis_index("tp")
    other = 1 - core
    seqs, heads, kl = query_latent.shape
    rope = query_rotary.shape[-1]
    cache_len = cache.shape[1]
    width = res_hbm.shape[1]
    extra = rows_all.shape[-1] - width
    half_fe = eg.shape[-1]
    fd = dg.shape[-1]
    inner = inner_size(n)
    outer = n // inner
    plane_rows = inner * seqs
    zo = lax.div(me, inner)
    xi = lax.rem(me, inner)
    upper = lax.div(2 * zo, outer)

    def far(k):
        down_order = outer - 1 - k
        down_order = down_order - jnp.where(down_order <= zo, 1, 0)
        up_order = k + jnp.where(zo <= k, 1, 0)
        return down_order + upper * (up_order - down_order)

    others = [far(k) for k in range(outer - 1)]

    def mate(d):
        return zo * inner + lax.rem(xi + d, inner)

    barrier = pltpu.get_barrier_semaphore()

    def greet(d, carry):
        peer = lax.rem(me + d, n)
        pl.semaphore_signal(barrier, inc=1, device_id={"ep": peer}, device_id_type=MESH)
        return carry

    lax.fori_loop(1, n, greet, 0)
    pl.semaphore_signal(barrier, inc=1, device_id={"tp": other}, device_id_type=MESH)

    own_down = down.at[pl.ds(pl.multiple_of(core * half_fe, half_fe), half_fe)]
    names = {}

    def load(name, a, b):
        c = pltpu.make_async_copy(a, b, in_sem.at[len(names)])
        c.start()
        names[name] = c

    load("qr", qr_hbm, query_rotary)
    load("rn", rn_hbm, rotary_new)
    load("ql", ql_hbm, query_latent)
    load("ln", ln_hbm, latent_new)
    load("rc", rc_hbm, rotary_cache)
    cache_copies = [
        pltpu.make_async_copy(cache_hbm.at[s], cache.at[s], cache_sem.at[s]) for s in range(seqs)
    ]
    for c in cache_copies:
        c.start()
    load("res", res_hbm, rows_all.at[me, :, pl.ds(0, width)])
    load("ids", ids_hbm, ids)
    load("rs", rs_hbm, route_scores)
    load("vu", vu_hbm, vu)
    load("op", op_hbm, op)
    load("ag", ag_hbm, attn_gain)
    load("mg", mg_hbm, mix_gate)
    load("eg", eg_hbm.at[0], eg.at[core])
    load("eu", eu_hbm.at[0], eu.at[core])
    load("ed", ed_hbm.at[0], own_down)
    load("dg", dg_hbm, dg)
    load("du", du_hbm, du)
    load("dd", dd_hbm, down.at[pl.ds(2 * half_fe, fd)])
    load("og", og_hbm, out_gain)

    half = rope // 2
    lane = lax.broadcasted_iota(jnp.int32, (seqs, rope), 1)
    row = lax.broadcasted_iota(jnp.int32, (seqs, rope), 0)
    pos = jnp.zeros((seqs, rope), F32)
    for s in range(seqs):
        pos = jnp.where(row == s, lengths[s].astype(F32), pos)
    inv_freq = jnp.exp(lax.rem(lane, half).astype(F32) * (-math.log(ROPE_BASE) / half))
    angles = pos * inv_freq
    cosine = jnp.cos(angles)
    sine = jnp.sin(angles)
    ra = lax.broadcasted_iota(jnp.int32, (rope, rope), 0)
    rb = lax.broadcasted_iota(jnp.int32, (rope, rope), 1)
    swap = jnp.where(ra + half == rb, 1.0, jnp.where(ra == rb + half, -1.0, 0.0)).astype(BF16)
    for name in ("qr", "rn", "ql", "ln", "rc"):
        names[name].wait()
    q_rot = query_rotary[...].astype(F32).reshape(seqs * heads, rope)
    q_swap = dot(q_rot.astype(BF16), swap).reshape(seqs, heads, rope)
    q_rot = q_rot.reshape(seqs, heads, rope)
    k_rot = rotary_new[...]
    k_turn = (k_rot.astype(F32) * cosine + dot(k_rot, swap) * sine).astype(BF16).astype(F32)
    ln_all = latent_new[...].astype(F32)
    score_scale = (NOPE + rope) ** (-0.5)
    t_idx = lax.broadcasted_iota(jnp.int32, (heads, cache_len), 1)

    score_rows, own_rows_all = [], []
    for s in range(seqs):
        q_turn = (q_rot[s] * cosine[s : s + 1] + q_swap[s] * sine[s : s + 1]).astype(BF16)
        ql = query_latent[s]
        own_rows_all.append(
            row_sum(ql.astype(F32) * ln_all[s : s + 1])
            + row_sum(q_turn.astype(F32) * k_turn[s : s + 1])
        )
        rot_part = dot(q_turn, rotary_cache[s])
        cache_copies[s].wait()
        part = dot_nt(ql, cache[s]) + rot_part
        score_rows.append(jnp.where(t_idx < lengths[s], part, -jnp.inf))
    own = jnp.concatenate(own_rows_all, 0) * score_scale
    scores = jnp.concatenate(score_rows, 0) * score_scale

    names["ids"].wait()
    names["rs"].wait()
    sc = route_scores[...]
    share = sc / row_sum(sc)
    e_lane = lax.broadcasted_iota(jnp.int32, (seqs, extra), 1)
    low = e_lane >= n
    e_idx = jnp.where(low, e_lane - n, e_lane)
    coef = jnp.zeros((seqs, extra), F32)
    for k in range(ids.shape[1]):
        coef = coef + jnp.where(e_idx == ids[:, k : k + 1], share[:, k : k + 1], 0.0)
    high = coef.astype(BF16)
    coef = jnp.where(low, coef - high.astype(F32), high.astype(F32)).astype(BF16)
    rows_all[me, :, width:] = coef

    pl.semaphore_wait(barrier, n)

    def row_copy(block, sem, target):
        return pltpu.make_async_remote_copy(
            src_ref=rows_all.at[block],
            dst_ref=rows_all.at[block],
            send_sem=r_send,
            recv_sem=sem,
            device_id={"ep": target},
            device_id_type=MESH,
        )

    def to_plane(p):
        block = p * inner + xi

        def send(d, carry):
            row_copy(block, r_plane.at[p], mate(d)).start()
            return carry

        lax.fori_loop(1, inner, send, 0)

    names["res"].wait()
    for p in others:
        row_copy(me, r_line.at[zo], p * inner + xi).start()
    to_plane(zo)

    pairs = [(eg_hbm.at[0], eg.at[core]), (eu_hbm.at[0], eu.at[core]), (ed_hbm.at[0], own_down)]
    w_copies = [
        pltpu.make_async_remote_copy(
            src_ref=a,
            dst_ref=b,
            send_sem=w_send.at[k],
            recv_sem=w_recv.at[k],
            device_id={"tp": other},
            device_id_type=MESH,
        )
        for k, (a, b) in enumerate(pairs)
    ]
    for c in w_copies:
        c.start()

    top = jnp.maximum(jnp.max(scores, -1, keepdims=True), own)
    probs = jnp.exp(scores - top)
    own_p = jnp.exp(own - top)
    total = row_sum(probs) + own_p
    weights = probs / total
    own_w = (own_p / total).astype(BF16).astype(F32)
    for s in range(seqs):
        at = slice(s * heads, (s + 1) * heads)
        lat[at, :] = dot(weights[at].astype(BF16), cache[s]) + own_w[at] * ln_all[s : s + 1]

    names["vu"].wait()
    wide = dot_nt(lat[...].astype(BF16), vu[...])
    hv = wide.shape[1]
    vdim = hv // heads
    wide = wide.reshape(seqs, heads, hv)
    h_row = lax.broadcasted_iota(jnp.int32, wide.shape, 1)
    h_lane = lax.broadcasted_iota(jnp.int32, wide.shape, 2)
    own_head = (h_lane >= h_row * vdim) & (h_lane < (h_row + 1) * vdim)
    heads_all[me] = jnp.sum(jnp.where(own_head, wide, 0.0), 1).astype(BF16)

    def head_copy(target):
        return pltpu.make_async_remote_copy(
            src_ref=heads_all.at[me],
            dst_ref=heads_all.at[me],
            send_sem=h_send,
            recv_sem=h_recv.at[zo],
            device_id={"ep": target},
            device_id_type=MESH,
        )

    for p in others:

        def send_line(i, carry):
            head_copy(p * inner + lax.rem(xi + i, inner)).start()
            return carry

        lax.fori_loop(0, inner, send_line, 0)

    def send_mate(d, carry):
        head_copy(mate(d)).start()
        return carry

    lax.fori_loop(1, inner, send_mate, 0)

    for p in reversed(others):
        row_copy(p * inner + xi, r_line.at[p], me).wait_recv()
        to_plane(p)
    order = [zo] + others[::-1]

    def block_wait(ref, send_sem, recv_sem):
        return pltpu.make_async_remote_copy(
            src_ref=ref,
            dst_ref=ref,
            send_sem=send_sem,
            recv_sem=recv_sem,
            device_id={"ep": me},
            device_id_type=MESH,
        )

    for name in ("op", "ag", "mg"):
        names[name].wait()
    tile = 512 if width % 512 == 0 else width
    tiles = width // tile
    slices = [slice(t * tile, (t + 1) * tile) for t in range(tiles)]

    def vector(ref, cols):
        return ref[cols].astype(F32).reshape(1, tile)

    def flat(ref, planes, cols):
        parts = []
        for p in planes:
            block = ref[pl.ds(p * inner, inner), :, cols].astype(F32)
            parts.append(block.reshape(plane_rows, block.shape[-1]))
        return parts[0] if len(parts) == 1 else jnp.concatenate(parts, 0)

    rows = group * plane_rows
    for c in range(outer // group):
        planes = order[c * group : (c + 1) * group]
        for k, p in enumerate(planes):
            own_plane = c == 0 and k == 0
            count = inner - 1 if own_plane else inner
            block_wait(heads_all.at[pl.ds(0, count)], h_send, h_recv.at[p]).wait_recv()
            block_wait(rows_all.at[pl.ds(0, inner - 1)], r_send, r_plane.at[p]).wait_recv()
        x = flat(heads_all, planes, slice(0, hv)).astype(BF16)
        total = jnp.zeros((rows, 1), F32)
        for cols in slices:
            attn = dot(x, op[:, cols]).astype(BF16).astype(F32)
            value = ALPHA * flat(rows_all, planes, cols) + attn
            wide_rows[:, cols] = value
            total = total + row_sum(value)
        center = total / width
        spread = jnp.zeros((rows, 1), F32)
        for cols in slices:
            spread = spread + row_sum(jnp.square(wide_rows[:, cols] - center))
        inv = lax.rsqrt(spread / width + EPS)
        gate = jnp.zeros((rows, 1), F32)
        for cols in slices:
            value = (wide_rows[:, cols] - center) * inv * vector(attn_gain, cols)
            value = value.astype(BF16)
            for k, p in enumerate(planes):
                at = pl.ds(pl.multiple_of(p * plane_rows, plane_rows), plane_rows)
                mixed[at, cols] = value[k * plane_rows : (k + 1) * plane_rows]
            gate = gate + row_sum(value.astype(F32) * vector(mix_gate, cols))
        blend = 1.0 / (1.0 + jnp.exp(-gate))
        tail = flat(rows_all, planes, slice(width, width + extra))
        c_lane = lax.broadcasted_iota(jnp.int32, (rows, extra), 1)
        weight = row_sum(jnp.where((c_lane == me) | (c_lane == me + n), tail, 0.0))
        s_lane = lax.broadcasted_iota(jnp.int32, (rows, 128), 1)
        both = jnp.where(s_lane == 0, weight, blend)
        for k, p in enumerate(planes):
            at = pl.ds(pl.multiple_of(p * plane_rows, plane_rows), plane_rows)
            scale[at, :] = both[k * plane_rows : (k + 1) * plane_rows]

    for name in ("eg", "eu", "ed", "dg", "du", "dd", "og"):
        names[name].wait()
    for c in w_copies:
        c.wait_recv()

    chunk = min(n * seqs, 128)

    def hidden(b, carry):
        at = pl.ds(pl.multiple_of(b * chunk, chunk), chunk)
        x = mixed[at, :]
        both = scale[at, :]
        weight, blend = both[:, 0:1], both[:, 1:2]
        for j in range(2):
            value = silu(dot(x, eg[j])) * dot(x, eu[j]) * weight
            hid[at, j * half_fe : (j + 1) * half_fe] = value.astype(BF16)
        value = silu(dot(x, dg[...])) * dot(x, du[...]) * blend
        hid[at, 2 * half_fe :] = value.astype(BF16)
        return carry

    lax.fori_loop(0, n * seqs // chunk, hidden, 0)

    def plane_copy(p, d, target):
        return pltpu.make_async_remote_copy(
            src_ref=sbuf.at[p, lax.rem(xi + d, inner)],
            dst_ref=rbuf.at[p, d],
            send_sem=s_send,
            recv_sem=s_plane.at[p],
            device_id={"ep": target},
            device_id_type=MESH,
        )

    for p in others + [zo]:
        at = pl.ds(pl.multiple_of(p * plane_rows, plane_rows), plane_rows)
        part = dot(hid[at, :], down[...])
        sbuf[p] = part.reshape(inner, seqs, width).astype(BF16)

        def send(d, carry):
            plane_copy(p, d, mate(d)).start()
            return carry

        lax.fori_loop(1, inner, send, 0)

    def plane_sum(p, start):
        block_wait(rbuf.at[p, pl.ds(1, inner - 1)], s_send, s_plane.at[p]).wait_recv()

        def one(d, total):
            return total + rbuf[p, d].astype(F32)

        return lax.fori_loop(1, inner, one, start, unroll=inner <= 4)

    for p in others:
        zbuf[p] = plane_sum(p, sbuf[p, xi].astype(F32)).astype(BF16)
        pltpu.make_async_remote_copy(
            src_ref=zbuf.at[p],
            dst_ref=zrecv.at[zo],
            send_sem=s_send,
            recv_sem=s_line,
            device_id={"ep": p * inner + xi},
            device_id_type=MESH,
        ).start()

    pair = mixed[pl.ds(pl.multiple_of(lax.div(me, 2) * 2 * seqs, 2 * seqs), 2 * seqs), :]
    pair = pair.astype(F32).reshape(2, seqs, width)
    odd = lax.rem(me, 2).astype(F32)
    start = ALPHA * (pair[0] + odd * (pair[1] - pair[0]))
    total = plane_sum(zo, start + sbuf[zo, xi].astype(F32))
    if outer > 1:
        block_wait(zrecv.at[pl.ds(0, outer - 1)], s_send, s_line).wait_recv()
    for p in others:
        total = total + zrecv[p].astype(F32)
    center = row_sum(total) / width
    shifted = total - center
    spread = row_sum(jnp.square(shifted)) / width
    gain = out_gain[...].astype(F32).reshape(1, width)
    out[...] = (shifted * lax.rsqrt(spread + EPS) * gain).astype(BF16)

    block_wait(rows_all.at[pl.ds(0, n - 1)], r_send, r_line.at[0]).wait_send()
    block_wait(heads_all.at[pl.ds(0, n - 1)], h_send, h_recv.at[0]).wait_send()
    for p in others:
        block_wait(rbuf.at[p], s_send, s_line).wait_send()
    block_wait(rbuf.at[zo, pl.ds(0, inner - 1)], s_send, s_line).wait_send()
    for c in w_copies:
        c.wait_send()


def on_device(
    n,
    residual,
    query_latent,
    query_rotary,
    latent_new,
    rotary_new,
    latent_cache,
    rotary_cache,
    lengths,
    value_up,
    out_proj,
    attn_gain,
    mix_gate,
    dense_w_gate,
    dense_w_up,
    dense_w_down,
    expert_ids,
    expert_scores,
    expert_gate,
    expert_up,
    expert_down,
    out_gain,
):
    seqs, width = residual.shape
    heads = query_latent.shape[1]
    vu = value_up.transpose(1, 2, 0).reshape(-1, value_up.shape[0])
    rotary_turned = rotary_cache.transpose(0, 2, 1)
    extra = -(-2 * n // 128) * 128
    inner = inner_size(n)
    outer = n // inner
    group = max(1, min(outer, 128 // (inner * seqs)))
    while outer % group:
        group -= 1
    hbm = pl.BlockSpec(memory_space=pl.ANY)
    smem = pl.BlockSpec(memory_space=pltpu.SMEM)
    dma = pltpu.SemaphoreType.DMA
    block = (outer, inner, seqs, width)
    half_fe = expert_gate.shape[-1]
    fd = dense_w_gate.shape[-1]
    return pl.pallas_call(
        functools.partial(kernel, n, group),
        out_shape=pltpu.VMEM((seqs, width), BF16),
        in_specs=[smem] + [hbm] * 20,
        out_specs=pl.BlockSpec(memory_space=VMEM),
        scratch_shapes=[
            VMEM(query_rotary.shape, BF16),
            VMEM(rotary_new.shape, BF16),
            VMEM(query_latent.shape, BF16),
            VMEM(latent_new.shape, BF16),
            VMEM(rotary_turned.shape, BF16),
            VMEM(latent_cache.shape, BF16),
            VMEM(expert_ids.shape, jnp.int32),
            VMEM(expert_scores.shape, F32),
            VMEM(vu.shape, BF16),
            VMEM(out_proj.shape, BF16),
            VMEM(attn_gain.shape, BF16),
            VMEM(mix_gate.shape, BF16),
            VMEM((2,) + expert_gate.shape[1:], BF16),
            VMEM((2,) + expert_up.shape[1:], BF16),
            VMEM((2 * half_fe + fd, width), BF16),
            VMEM(dense_w_gate.shape, BF16),
            VMEM(dense_w_up.shape, BF16),
            VMEM(out_gain.shape, BF16),
            VMEM((seqs * heads, latent_cache.shape[-1]), F32),
            VMEM((n, seqs, width + extra), BF16),
            VMEM((n, seqs, vu.shape[0]), BF16),
            VMEM((group * inner * seqs, width), F32),
            VMEM((n * seqs, width), BF16),
            VMEM((n * seqs, 128), F32),
            VMEM((n * seqs, 2 * half_fe + fd), BF16),
            VMEM(block, BF16),
            VMEM(block, BF16),
            VMEM((outer, seqs, width), BF16),
            VMEM((outer, seqs, width), BF16),
            dma((19,)),
            dma((seqs,)),
            dma((3,)),
            dma((3,)),
            dma,
            dma((outer,)),
            dma((outer,)),
            dma,
            dma((outer,)),
            dma,
            dma((outer,)),
            dma,
        ],
        compiler_params=pltpu.CompilerParams(
            collective_id=0, has_side_effects=True, vmem_limit_bytes=60 * 1024 * 1024
        ),
    )(
        lengths,
        query_rotary,
        rotary_new,
        query_latent,
        latent_new,
        rotary_turned,
        latent_cache,
        residual,
        expert_ids,
        expert_scores,
        vu,
        out_proj,
        attn_gain,
        mix_gate,
        expert_gate,
        expert_up,
        expert_down,
        dense_w_gate,
        dense_w_up,
        dense_w_down,
        out_gain,
    )


def solution(mesh):
    rows = P(("ep", "tp"), None)
    rows3 = P(("ep", "tp"), None, None)
    return jax.shard_map(
        functools.partial(on_device, mesh.shape["ep"]),
        mesh=mesh,
        in_specs=(
            rows,
            rows3,
            rows3,
            rows,
            rows,
            rows3,
            rows3,
            P(("ep", "tp")),
            P(),
            P(),
            P(),
            P(),
            P(None, "ep"),
            P(None, "ep"),
            P("ep", None),
            rows,
            rows,
            P("ep", None, "tp"),
            P("ep", None, "tp"),
            P("ep", "tp", None),
            P(),
        ),
        out_specs=rows,
        check_vma=False,
    )
```

```python
import functools
import math

import jax
import jax.numpy as jnp
from jax import lax
from jax.experimental import pallas as pl
from jax.experimental.pallas import tpu as pltpu
from jax.sharding import PartitionSpec as P

NOPE = 64
ALPHA = 8.0**0.25
EPS = 1e-06
ROPE_BASE = 10000.0
F32 = jnp.float32
BF16 = jnp.bfloat16
MESH = pl.DeviceIdType.MESH
VMEM = pltpu.VMEM


def inner_size(n):
    size = 1
    while size * size < n:
        size *= 2
    return size if n % size == 0 else n


def silu(value):
    return value / (1.0 + jnp.exp(-value))


def dot(a, b):
    return jnp.dot(a, b, preferred_element_type=F32)


def dot_nt(a, b):
    return lax.dot_general(a, b, (((1,), (1,)), ((), ())), preferred_element_type=F32)


def row_sum(value):
    return jnp.sum(value, -1, keepdims=True)


def kernel(
    n,
    groups,
    len_hbm,
    qr_hbm,
    rn_hbm,
    ql_hbm,
    ln_hbm,
    rc_hbm,
    cache_hbm,
    res_hbm,
    ids_hbm,
    rs_hbm,
    vu_hbm,
    op_hbm,
    ag_hbm,
    mg_hbm,
    eg_hbm,
    eu_hbm,
    ed_hbm,
    dg_hbm,
    du_hbm,
    dd_hbm,
    og_hbm,
    out,
    lengths,
    query_rotary,
    rotary_new,
    query_latent,
    latent_new,
    rotary_cache,
    cache,
    ids,
    route_scores,
    vu,
    op,
    attn_gain,
    mix_gate,
    eg,
    eu,
    down,
    dg,
    du,
    out_gain,
    lat,
    rows_all,
    heads_all,
    wide_rows,
    mixed,
    own_mixed,
    hid,
    sbuf,
    rbuf,
    zbuf,
    zrecv,
    in_sem,
    cache_sem,
    w_send,
    w_recv,
    r_send,
    r_line,
    r_plane,
    h_send,
    h_recv,
    s_send,
    s_plane,
    s_line,
    ready,
):
    me = lax.axis_index("ep")
    core = lax.axis_index("tp")
    other = 1 - core
    seqs, heads, kl = query_latent.shape
    rope = query_rotary.shape[-1]
    cache_len = cache.shape[1]
    width = res_hbm.shape[1]
    extra = rows_all.shape[-1] - width
    half_fe = eg.shape[-1]
    fd = dg.shape[-1]
    inner = inner_size(n)
    outer = n // inner
    plane_rows = inner * seqs
    zo = lax.div(me, inner)
    xi = lax.rem(me, inner)
    upper = lax.div(2 * zo, outer)

    def descend(k):
        p = outer - 1 - k
        return p - jnp.where(p <= zo, 1, 0)

    def far(k):
        first = descend(k)
        lower = first + lax.min(zo, 1) * ((descend(k - 1) if k else 0) - first)
        return lower + upper * (k + jnp.where(zo <= k, 1, 0) - lower)

    others = [far(k) for k in range(outer - 1)]

    def mate(d):
        return zo * inner + lax.rem(xi + d, inner)

    barrier = pltpu.get_barrier_semaphore()

    def greet(sem, peer):
        pl.semaphore_signal(sem, inc=1, device_id={"ep": peer}, device_id_type=MESH)

    def greet_mate(d, carry):
        greet(barrier, mate(d))
        return carry

    for p in others:
        greet(barrier, p * inner + xi)
    lax.fori_loop(1, inner, greet_mate, 0)
    pl.semaphore_signal(barrier, inc=1, device_id={"tp": other}, device_id_type=MESH)

    own_down = down.at[pl.ds(pl.multiple_of(core * half_fe, half_fe), half_fe)]
    names = {}

    def load(name, a, b):
        c = pltpu.make_async_copy(a, b, in_sem.at[len(names)])
        c.start()
        names[name] = c

    load("len", len_hbm, lengths)
    load("qr", qr_hbm, query_rotary)
    load("rn", rn_hbm, rotary_new)
    load("ql", ql_hbm, query_latent)
    load("ln", ln_hbm, latent_new)
    load("rc", rc_hbm, rotary_cache)
    load("res", res_hbm, rows_all.at[me, :, pl.ds(0, width)])
    load("ids", ids_hbm, ids)
    load("rs", rs_hbm, route_scores)
    cache_copies = [
        pltpu.make_async_copy(cache_hbm.at[s], cache.at[s], cache_sem.at[s]) for s in range(seqs)
    ]
    for c in cache_copies:
        c.start()

    half = rope // 2
    names["len"].wait()
    lane = lax.broadcasted_iota(jnp.int32, (seqs, rope), 1)
    row = lax.broadcasted_iota(jnp.int32, (seqs, rope), 0)
    pos = jnp.zeros((seqs, rope), F32)
    for s in range(seqs):
        pos = jnp.where(row == s, lengths[s].astype(F32), pos)
    inv_freq = jnp.exp(lax.rem(lane, half).astype(F32) * (-math.log(ROPE_BASE) / half))
    angles = pos * inv_freq
    cosine = jnp.cos(angles)
    sine = jnp.sin(angles)
    ra = lax.broadcasted_iota(jnp.int32, (rope, rope), 0)
    rb = lax.broadcasted_iota(jnp.int32, (rope, rope), 1)
    swap = jnp.where(ra + half == rb, 1.0, jnp.where(ra == rb + half, -1.0, 0.0)).astype(BF16)
    for name in ("qr", "rn", "ql", "ln", "rc"):
        names[name].wait()
    q_rot = query_rotary[...].astype(F32).reshape(seqs * heads, rope)
    q_swap = dot(q_rot.astype(BF16), swap).reshape(seqs, heads, rope)
    q_rot = q_rot.reshape(seqs, heads, rope)
    k_rot = rotary_new[...]
    k_turn = (k_rot.astype(F32) * cosine + dot(k_rot, swap) * sine).astype(BF16).astype(F32)
    ln_all = latent_new[...].astype(F32)
    score_scale = (NOPE + rope) ** (-0.5)
    t_idx = lax.broadcasted_iota(jnp.int32, (heads, cache_len), 1)

    names["ids"].wait()
    names["rs"].wait()
    sc = route_scores[...]
    share = sc / row_sum(sc)
    e_lane = lax.broadcasted_iota(jnp.int32, (seqs, extra), 1)
    low = e_lane >= n
    e_idx = jnp.where(low, e_lane - n, e_lane)
    coef = jnp.zeros((seqs, extra), F32)
    for k in range(ids.shape[1]):
        coef = coef + jnp.where(e_idx == ids[:, k : k + 1], share[:, k : k + 1], 0.0)
    high = coef.astype(BF16)
    coef = jnp.where(low, coef - high.astype(F32), high.astype(F32)).astype(BF16)
    rows_all[me, :, width:] = coef

    def row_copy(block, sem, target):
        return pltpu.make_async_remote_copy(
            src_ref=rows_all.at[block],
            dst_ref=rows_all.at[block],
            send_sem=r_send,
            recv_sem=sem,
            device_id={"ep": target},
            device_id_type=MESH,
        )

    def to_plane(p):
        block = p * inner + xi

        def send(d, carry):
            row_copy(block, r_plane.at[p], mate(d)).start()
            return carry

        lax.fori_loop(1, inner, send, 0)

    pairs = [(eg_hbm.at[0], eg.at[core]), (eu_hbm.at[0], eu.at[core]), (ed_hbm.at[0], own_down)]
    w_copies = [
        pltpu.make_async_remote_copy(
            src_ref=a,
            dst_ref=b,
            send_sem=w_send.at[k],
            recv_sem=w_recv.at[k],
            device_id={"tp": other},
            device_id_type=MESH,
        )
        for k, (a, b) in enumerate(pairs)
    ]
    def announce():
        pl.semaphore_wait(barrier, outer + inner - 1)
        for p in others:
            greet(ready, p * inner + xi)
        for p in others:
            row_copy(me, r_line.at[zo], p * inner + xi).start()
        to_plane(zo)
        for c in w_copies:
            c.start()

    names["res"].wait()
    @pl.when(upper == 1)
    def _():
        announce()

    score_rows, own_rows_all = [], []
    for s in range(seqs):
        q_turn = (q_rot[s] * cosine[s : s + 1] + q_swap[s] * sine[s : s + 1]).astype(BF16)
        ql = query_latent[s]
        own_rows_all.append(
            row_sum(ql.astype(F32) * ln_all[s : s + 1])
            + row_sum(q_turn.astype(F32) * k_turn[s : s + 1])
        )
        rot_part = dot(q_turn, rotary_cache[s])
        cache_copies[s].wait()
        part = dot_nt(ql, cache[s]) + rot_part
        score_rows.append(jnp.where(t_idx < lengths[s], part, -jnp.inf))
    load("vu", vu_hbm, vu)
    load("op", op_hbm, op)
    load("ag", ag_hbm, attn_gain)
    load("mg", mg_hbm, mix_gate)
    load("eg", eg_hbm.at[0], eg.at[core])
    load("eu", eu_hbm.at[0], eu.at[core])
    load("ed", ed_hbm.at[0], own_down)
    load("dg", dg_hbm, dg)
    load("du", du_hbm, du)
    load("dd", dd_hbm, down.at[pl.ds(2 * half_fe, fd)])
    load("og", og_hbm, out_gain)
    own = jnp.concatenate(own_rows_all, 0) * score_scale
    scores = jnp.concatenate(score_rows, 0) * score_scale

    @pl.when(upper == 0)
    def _():
        announce()

    top = jnp.maximum(jnp.max(scores, -1, keepdims=True), own)
    probs = jnp.exp(scores - top)
    own_p = jnp.exp(own - top)
    total = row_sum(probs) + own_p
    weights = probs / total
    own_w = (own_p / total).astype(BF16).astype(F32)
    for s in range(seqs):
        at = slice(s * heads, (s + 1) * heads)
        lat[at, :] = dot(weights[at].astype(BF16), cache[s]) + own_w[at] * ln_all[s : s + 1]

    names["vu"].wait()
    wide = dot_nt(lat[...].astype(BF16), vu[...])
    hv = wide.shape[1]
    vdim = hv // heads
    wide = wide.reshape(seqs, heads, hv)
    h_row = lax.broadcasted_iota(jnp.int32, wide.shape, 1)
    h_lane = lax.broadcasted_iota(jnp.int32, wide.shape, 2)
    own_head = (h_lane >= h_row * vdim) & (h_lane < (h_row + 1) * vdim)
    heads_all[me] = jnp.sum(jnp.where(own_head, wide, 0.0), 1).astype(BF16)

    if outer > 1:
        pl.semaphore_wait(ready, outer - 1)

    def head_copy(target):
        return pltpu.make_async_remote_copy(
            src_ref=heads_all.at[me],
            dst_ref=heads_all.at[me],
            send_sem=h_send,
            recv_sem=h_recv.at[zo],
            device_id={"ep": target},
            device_id_type=MESH,
        )

    for p in others:

        def send_line(i, carry):
            head_copy(p * inner + lax.rem(xi + i, inner)).start()
            return carry

        lax.fori_loop(0, inner, send_line, 0)

    def send_mate(d, carry):
        head_copy(mate(d)).start()
        return carry

    lax.fori_loop(1, inner, send_mate, 0)

    for p in others:
        row_copy(p * inner + xi, r_line.at[p], me).wait_recv()
        to_plane(p)
    order = others + [zo]

    def block_wait(ref, send_sem, recv_sem):
        return pltpu.make_async_remote_copy(
            src_ref=ref,
            dst_ref=ref,
            send_sem=send_sem,
            recv_sem=recv_sem,
            device_id={"ep": me},
            device_id_type=MESH,
        )

    for name in ("op", "ag", "mg"):
        names[name].wait()
    tile = 512 if width % 512 == 0 else width
    tiles = width // tile
    slices = [slice(t * tile, (t + 1) * tile) for t in range(tiles)]

    def vector(ref, cols):
        return ref[cols].astype(F32).reshape(1, tile)

    def flat(ref, planes, cols):
        parts = []
        for p in planes:
            block = ref[pl.ds(p * inner, inner), :, cols].astype(F32)
            parts.append(block.reshape(plane_rows, block.shape[-1]))
        return parts[0] if len(parts) == 1 else jnp.concatenate(parts, 0)

    def plane_copy(p, d, target):
        return pltpu.make_async_remote_copy(
            src_ref=sbuf.at[p, lax.rem(xi + d, inner)],
            dst_ref=rbuf.at[p, d],
            send_sem=s_send,
            recv_sem=s_plane.at[p],
            device_id={"ep": target},
            device_id_type=MESH,
        )

    chunks = len(groups)
    for c in range(chunks):
        group = groups[c]
        rows = group * plane_rows
        planes = order[sum(groups[:c]) : sum(groups[: c + 1])]
        for k, p in enumerate(planes):
            own_plane = c == chunks - 1 and k == group - 1
            count = inner - 1 if own_plane else inner
            block_wait(heads_all.at[pl.ds(0, count)], h_send, h_recv.at[p]).wait_recv()
            block_wait(rows_all.at[pl.ds(0, inner - 1)], r_send, r_plane.at[p]).wait_recv()
        x = flat(heads_all, planes, slice(0, hv)).astype(BF16)
        total = jnp.zeros((rows, 1), F32)
        for cols in slices:
            attn = dot(x, op[:, cols]).astype(BF16).astype(F32)
            value = ALPHA * flat(rows_all, planes, cols) + attn
            wide_rows[:rows, cols] = value
            total = total + row_sum(value)
        center = total / width
        spread = jnp.zeros((rows, 1), F32)
        for cols in slices:
            spread = spread + row_sum(jnp.square(wide_rows[:rows, cols] - center))
        inv = lax.rsqrt(spread / width + EPS)
        gate = jnp.zeros((rows, 1), F32)
        for cols in slices:
            value = (wide_rows[:rows, cols] - center) * inv * vector(attn_gain, cols)
            value = value.astype(BF16)
            mixed[:rows, cols] = value
            if c == chunks - 1:
                own_mixed[:, cols] = value[rows - plane_rows :]
            gate = gate + row_sum(value.astype(F32) * vector(mix_gate, cols))
        blend = 1.0 / (1.0 + jnp.exp(-gate))
        tail = flat(rows_all, planes, slice(width, width + extra))
        c_lane = lax.broadcasted_iota(jnp.int32, (rows, extra), 1)
        weight = row_sum(jnp.where((c_lane == me) | (c_lane == me + n), tail, 0.0))

        if c == 0:
            for name in ("eg", "eu", "ed", "dg", "du", "dd", "og"):
                names[name].wait()
            for w in w_copies:
                w.wait_recv()
        x = mixed[:rows, :]
        for j in range(2):
            value = silu(dot(x, eg[j])) * dot(x, eu[j]) * weight
            hid[:rows, j * half_fe : (j + 1) * half_fe] = value.astype(BF16)
        value = silu(dot(x, dg[...])) * dot(x, du[...]) * blend
        hid[:rows, 2 * half_fe :] = value.astype(BF16)

        for cols in slices:
            part = dot(hid[:rows, :], down[:, cols])
            for k, p in enumerate(planes):
                block = part[k * plane_rows : (k + 1) * plane_rows].reshape(inner, seqs, tile)
                sbuf[p, :, :, cols] = block.astype(BF16)
        for p in planes:

            def send(d, carry):
                plane_copy(p, d, mate(d)).start()
                return carry

            lax.fori_loop(1, inner, send, 0)

    def plane_sum(p, start):
        block_wait(rbuf.at[p, pl.ds(1, inner - 1)], s_send, s_plane.at[p]).wait_recv()

        def one(d, total):
            return total + rbuf[p, d].astype(F32)

        return lax.fori_loop(1, inner, one, start, unroll=inner <= 4)

    for p in others:
        zbuf[p] = plane_sum(p, sbuf[p, xi].astype(F32)).astype(BF16)
        pltpu.make_async_remote_copy(
            src_ref=zbuf.at[p],
            dst_ref=zrecv.at[zo],
            send_sem=s_send,
            recv_sem=s_line,
            device_id={"ep": p * inner + xi},
            device_id_type=MESH,
        ).start()

    at = pl.ds(pl.multiple_of(lax.div(xi, 2) * 2 * seqs, 2 * seqs), 2 * seqs)
    pair = own_mixed[at, :]
    pair = pair.astype(F32).reshape(2, seqs, width)
    odd = lax.rem(xi, 2).astype(F32)
    start = ALPHA * (pair[0] + odd * (pair[1] - pair[0]))
    total = plane_sum(zo, start + sbuf[zo, xi].astype(F32))
    if outer > 1:
        block_wait(zrecv.at[pl.ds(0, outer - 1)], s_send, s_line).wait_recv()
    for p in others:
        total = total + zrecv[p].astype(F32)
    center = row_sum(total) / width
    shifted = total - center
    spread = row_sum(jnp.square(shifted)) / width
    gain = out_gain[...].astype(F32).reshape(1, width)
    out[...] = (shifted * lax.rsqrt(spread + EPS) * gain).astype(BF16)

    block_wait(rows_all.at[pl.ds(0, n - 1)], r_send, r_line.at[0]).wait_send()
    block_wait(heads_all.at[pl.ds(0, n - 1)], h_send, h_recv.at[0]).wait_send()
    for p in others:
        block_wait(rbuf.at[p], s_send, s_line).wait_send()
    block_wait(rbuf.at[zo, pl.ds(0, inner - 1)], s_send, s_line).wait_send()
    for c in w_copies:
        c.wait_send()


def on_device(
    n,
    residual,
    query_latent,
    query_rotary,
    latent_new,
    rotary_new,
    latent_cache,
    rotary_cache,
    lengths,
    value_up,
    out_proj,
    attn_gain,
    mix_gate,
    dense_w_gate,
    dense_w_up,
    dense_w_down,
    expert_ids,
    expert_scores,
    expert_gate,
    expert_up,
    expert_down,
    out_gain,
):
    seqs, width = residual.shape
    heads = query_latent.shape[1]
    vu = value_up.transpose(1, 2, 0).reshape(-1, value_up.shape[0])
    rotary_turned = rotary_cache.transpose(0, 2, 1)
    extra = -(-2 * n // 128) * 128
    inner = inner_size(n)
    outer = n // inner
    most = max(1, 128 // (inner * seqs))
    groups = [1]
    while sum(groups) < outer:
        groups.append(min(most, outer - sum(groups)))
    top = max(groups) * inner * seqs
    hbm = pl.BlockSpec(memory_space=pl.ANY)
    dma = pltpu.SemaphoreType.DMA
    block = (outer, inner, seqs, width)
    half_fe = expert_gate.shape[-1]
    fd = dense_w_gate.shape[-1]
    return pl.pallas_call(
        functools.partial(kernel, n, tuple(groups)),
        out_shape=pltpu.VMEM((seqs, width), BF16),
        in_specs=[hbm] * 21,
        out_specs=pl.BlockSpec(memory_space=VMEM),
        scratch_shapes=[
            pltpu.SMEM(lengths.shape, jnp.int32),
            VMEM(query_rotary.shape, BF16),
            VMEM(rotary_new.shape, BF16),
            VMEM(query_latent.shape, BF16),
            VMEM(latent_new.shape, BF16),
            VMEM(rotary_turned.shape, BF16),
            VMEM(latent_cache.shape, BF16),
            VMEM(expert_ids.shape, jnp.int32),
            VMEM(expert_scores.shape, F32),
            VMEM(vu.shape, BF16),
            VMEM(out_proj.shape, BF16),
            VMEM(attn_gain.shape, BF16),
            VMEM(mix_gate.shape, BF16),
            VMEM((2,) + expert_gate.shape[1:], BF16),
            VMEM((2,) + expert_up.shape[1:], BF16),
            VMEM((2 * half_fe + fd, width), BF16),
            VMEM(dense_w_gate.shape, BF16),
            VMEM(dense_w_up.shape, BF16),
            VMEM(out_gain.shape, BF16),
            VMEM((seqs * heads, latent_cache.shape[-1]), F32),
            VMEM((n, seqs, width + extra), BF16),
            VMEM((n, seqs, vu.shape[0]), BF16),
            VMEM((top, width), F32),
            VMEM((top, width), BF16),
            VMEM((inner * seqs, width), BF16),
            VMEM((top, 2 * half_fe + fd), BF16),
            VMEM(block, BF16),
            VMEM(block, BF16),
            VMEM((outer, seqs, width), BF16),
            VMEM((outer, seqs, width), BF16),
            dma((20,)),
            dma((seqs,)),
            dma((3,)),
            dma((3,)),
            dma,
            dma((outer,)),
            dma((outer,)),
            dma,
            dma((outer,)),
            dma,
            dma((outer,)),
            dma,
            pltpu.SemaphoreType.REGULAR,
        ],
        compiler_params=pltpu.CompilerParams(
            collective_id=0, has_side_effects=True, vmem_limit_bytes=60 * 1024 * 1024
        ),
    )(
        lengths,
        query_rotary,
        rotary_new,
        query_latent,
        latent_new,
        rotary_turned,
        latent_cache,
        residual,
        expert_ids,
        expert_scores,
        vu,
        out_proj,
        attn_gain,
        mix_gate,
        expert_gate,
        expert_up,
        expert_down,
        dense_w_gate,
        dense_w_up,
        dense_w_down,
        out_gain,
    )


def solution(mesh):
    rows = P(("ep", "tp"), None)
    rows3 = P(("ep", "tp"), None, None)
    return jax.shard_map(
        functools.partial(on_device, mesh.shape["ep"]),
        mesh=mesh,
        in_specs=(
            rows,
            rows3,
            rows3,
            rows,
            rows,
            rows3,
            rows3,
            P(("ep", "tp")),
            P(),
            P(),
            P(),
            P(),
            P(None, "ep"),
            P(None, "ep"),
            P("ep", None),
            rows,
            rows,
            P("ep", None, "tp"),
            P("ep", None, "tp"),
            P("ep", "tp", None),
            P(),
        ),
        out_specs=rows,
        check_vma=False,
    )
```

```python
import functools
import math

import jax
import jax.numpy as jnp
from jax import lax
from jax.experimental import pallas as pl
from jax.experimental.pallas import tpu as pltpu
from jax.sharding import PartitionSpec as P

NOPE = 64
ALPHA = 8.0**0.25
EPS = 1e-06
ROPE_BASE = 10000.0
F32 = jnp.float32
BF16 = jnp.bfloat16
MESH = pl.DeviceIdType.MESH
VMEM = pltpu.VMEM


def inner_size(n):
    size = 1
    while size * size < n:
        size *= 2
    return size if n % size == 0 else n


def silu(value):
    return value / (1.0 + jnp.exp(-value))


def dot(a, b):
    return jnp.dot(a, b, preferred_element_type=F32)


def dot_nt(a, b):
    return lax.dot_general(a, b, (((1,), (1,)), ((), ())), preferred_element_type=F32)


def row_sum(value):
    return jnp.sum(value, -1, keepdims=True)


def kernel(
    n,
    groups,
    len_hbm,
    qr_hbm,
    rn_hbm,
    ql_hbm,
    ln_hbm,
    rc_hbm,
    cache_hbm,
    res_hbm,
    ids_hbm,
    rs_hbm,
    vu_hbm,
    op_hbm,
    ag_hbm,
    mg_hbm,
    eg_hbm,
    eu_hbm,
    ed_hbm,
    dg_hbm,
    du_hbm,
    dd_hbm,
    og_hbm,
    out,
    lengths,
    query_rotary,
    rotary_new,
    query_latent,
    latent_new,
    rotary_cache,
    cache,
    ids,
    route_scores,
    vu,
    op,
    attn_gain,
    mix_gate,
    eg,
    eu,
    down,
    dg,
    du,
    out_gain,
    lat,
    rows_all,
    heads_all,
    wide_rows,
    mixed,
    own_mixed,
    hid,
    sbuf,
    rbuf,
    zbuf,
    zrecv,
    in_sem,
    cache_sem,
    w_send,
    w_recv,
    r_send,
    r_line,
    r_plane,
    h_send,
    h_recv,
    s_send,
    s_plane,
    s_line,
    ready,
    obuf,
    yout,
    o_plane,
):
    me = lax.axis_index("ep")
    core = lax.axis_index("tp")
    other = 1 - core
    seqs, heads, kl = query_latent.shape
    rope = query_rotary.shape[-1]
    cache_len = cache.shape[1]
    width = res_hbm.shape[1]
    extra = rows_all.shape[-1] - width
    half_fe = eg.shape[-1]
    fd = dg.shape[-1]
    inner = inner_size(n)
    outer = n // inner
    plane_rows = inner * seqs
    zo = lax.div(me, inner)
    xi = lax.rem(me, inner)
    upper = lax.div(2 * zo, outer)

    def descend(k):
        p = outer - 1 - k
        return p - jnp.where(p <= zo, 1, 0)

    def far(k):
        first = descend(k)
        lower = first + lax.min(zo, 1) * ((descend(k - 1) if k else 0) - first)
        return lower + upper * (k + jnp.where(zo <= k, 1, 0) - lower)

    others = [far(k) for k in range(outer - 1)]

    def mate(d):
        return zo * inner + lax.rem(xi + d, inner)

    barrier = pltpu.get_barrier_semaphore()

    def greet(sem, peer):
        pl.semaphore_signal(sem, inc=1, device_id={"ep": peer}, device_id_type=MESH)

    def greet_mate(d, carry):
        greet(barrier, mate(d))
        return carry

    for p in others:
        greet(barrier, p * inner + xi)
    lax.fori_loop(1, inner, greet_mate, 0)
    pl.semaphore_signal(barrier, inc=1, device_id={"tp": other}, device_id_type=MESH)

    own_down = down.at[pl.ds(pl.multiple_of(core * half_fe, half_fe), half_fe)]
    names = {}

    def load(name, a, b):
        c = pltpu.make_async_copy(a, b, in_sem.at[len(names)])
        c.start()
        names[name] = c

    load("len", len_hbm, lengths)
    load("qr", qr_hbm, query_rotary)
    load("rn", rn_hbm, rotary_new)
    load("ql", ql_hbm, query_latent)
    load("ln", ln_hbm, latent_new)
    load("rc", rc_hbm, rotary_cache)
    load("res", res_hbm, rows_all.at[me, :, pl.ds(0, width)])
    load("ids", ids_hbm, ids)
    load("rs", rs_hbm, route_scores)
    cache_copies = [
        pltpu.make_async_copy(cache_hbm.at[s], cache.at[s], cache_sem.at[s]) for s in range(seqs)
    ]
    for c in cache_copies:
        c.start()

    half = rope // 2
    names["len"].wait()
    lane = lax.broadcasted_iota(jnp.int32, (seqs, rope), 1)
    row = lax.broadcasted_iota(jnp.int32, (seqs, rope), 0)
    pos = jnp.zeros((seqs, rope), F32)
    for s in range(seqs):
        pos = jnp.where(row == s, lengths[s].astype(F32), pos)
    inv_freq = jnp.exp(lax.rem(lane, half).astype(F32) * (-math.log(ROPE_BASE) / half))
    angles = pos * inv_freq
    cosine = jnp.cos(angles)
    sine = jnp.sin(angles)
    ra = lax.broadcasted_iota(jnp.int32, (rope, rope), 0)
    rb = lax.broadcasted_iota(jnp.int32, (rope, rope), 1)
    swap = jnp.where(ra + half == rb, 1.0, jnp.where(ra == rb + half, -1.0, 0.0)).astype(BF16)
    for name in ("qr", "rn", "ql", "ln", "rc"):
        names[name].wait()
    q_rot = query_rotary[...].astype(F32).reshape(seqs * heads, rope)
    q_swap = dot(q_rot.astype(BF16), swap).reshape(seqs, heads, rope)
    q_rot = q_rot.reshape(seqs, heads, rope)
    k_rot = rotary_new[...]
    k_turn = (k_rot.astype(F32) * cosine + dot(k_rot, swap) * sine).astype(BF16).astype(F32)
    ln_all = latent_new[...].astype(F32)
    score_scale = (NOPE + rope) ** (-0.5)
    t_idx = lax.broadcasted_iota(jnp.int32, (heads, cache_len), 1)

    names["ids"].wait()
    names["rs"].wait()
    sc = route_scores[...]
    share = sc / row_sum(sc)
    e_lane = lax.broadcasted_iota(jnp.int32, (seqs, extra), 1)
    low = e_lane >= n
    e_idx = jnp.where(low, e_lane - n, e_lane)
    coef = jnp.zeros((seqs, extra), F32)
    for k in range(ids.shape[1]):
        coef = coef + jnp.where(e_idx == ids[:, k : k + 1], share[:, k : k + 1], 0.0)
    high = coef.astype(BF16)
    coef = jnp.where(low, coef - high.astype(F32), high.astype(F32)).astype(BF16)
    rows_all[me, :, width:] = coef

    def row_copy(block, sem, target):
        return pltpu.make_async_remote_copy(
            src_ref=rows_all.at[block],
            dst_ref=rows_all.at[block],
            send_sem=r_send,
            recv_sem=sem,
            device_id={"ep": target},
            device_id_type=MESH,
        )

    def to_plane(p):
        block = p * inner + xi

        def send(d, carry):
            row_copy(block, r_plane.at[p], mate(d)).start()
            return carry

        lax.fori_loop(1, inner, send, 0)

    pairs = [(eg_hbm.at[0], eg.at[core]), (eu_hbm.at[0], eu.at[core]), (ed_hbm.at[0], own_down)]
    w_copies = [
        pltpu.make_async_remote_copy(
            src_ref=a,
            dst_ref=b,
            send_sem=w_send.at[k],
            recv_sem=w_recv.at[k],
            device_id={"tp": other},
            device_id_type=MESH,
        )
        for k, (a, b) in enumerate(pairs)
    ]
    def announce():
        pl.semaphore_wait(barrier, outer + inner - 1)
        for p in others:
            greet(ready, p * inner + xi)

        for p in others:
            row_copy(me, r_line.at[zo], p * inner + xi).start()
        to_plane(zo)
        for c in w_copies:
            c.start()

    names["res"].wait()
    @pl.when(upper == 1)
    def _():
        announce()

    score_rows, own_rows_all = [], []
    for s in range(seqs):
        q_turn = (q_rot[s] * cosine[s : s + 1] + q_swap[s] * sine[s : s + 1]).astype(BF16)
        ql = query_latent[s]
        own_rows_all.append(
            row_sum(ql.astype(F32) * ln_all[s : s + 1])
            + row_sum(q_turn.astype(F32) * k_turn[s : s + 1])
        )
        rot_part = dot(q_turn, rotary_cache[s])
        if s % 8 == 0:
            for c in cache_copies[s : s + 8]:
                c.wait()
        part = dot_nt(ql, cache[s]) + rot_part
        score_rows.append(jnp.where(t_idx < lengths[s], part, -jnp.inf))
    load("vu", vu_hbm, vu)
    load("op", op_hbm, op)
    load("ag", ag_hbm, attn_gain)
    load("mg", mg_hbm, mix_gate)
    load("eg", eg_hbm.at[0], eg.at[core])
    load("eu", eu_hbm.at[0], eu.at[core])
    load("ed", ed_hbm.at[0], own_down)
    load("dg", dg_hbm, dg)
    load("du", du_hbm, du)
    load("dd", dd_hbm, down.at[pl.ds(2 * half_fe, fd)])
    load("og", og_hbm, out_gain)
    own = jnp.concatenate(own_rows_all, 0) * score_scale
    scores = jnp.concatenate(score_rows, 0) * score_scale

    @pl.when(upper == 0)
    def _():
        announce()

    top = jnp.maximum(jnp.max(scores, -1, keepdims=True), own)
    probs = jnp.exp(scores - top)
    own_p = jnp.exp(own - top)
    total = row_sum(probs) + own_p
    weights = probs / total
    own_w = (own_p / total).astype(BF16).astype(F32)
    for s in range(seqs):
        at = slice(s * heads, (s + 1) * heads)
        lat[at, :] = dot(weights[at].astype(BF16), cache[s]) + own_w[at] * ln_all[s : s + 1]

    names["vu"].wait()
    wide = dot_nt(lat[...].astype(BF16), vu[...])
    hv = wide.shape[1]
    vdim = hv // heads
    wide = wide.reshape(seqs, heads, hv)
    h_row = lax.broadcasted_iota(jnp.int32, wide.shape, 1)
    h_lane = lax.broadcasted_iota(jnp.int32, wide.shape, 2)
    own_head = (h_lane >= h_row * vdim) & (h_lane < (h_row + 1) * vdim)
    heads_all[me] = jnp.sum(jnp.where(own_head, wide, 0.0), 1).astype(BF16)

    if outer > 1:
        pl.semaphore_wait(ready, outer - 1)

    def head_copy(target):
        return pltpu.make_async_remote_copy(
            src_ref=heads_all.at[me],
            dst_ref=heads_all.at[me],
            send_sem=h_send,
            recv_sem=h_recv.at[zo],
            device_id={"ep": target},
            device_id_type=MESH,
        )

    for p in others:

        def send_line(i, carry):
            head_copy(p * inner + lax.rem(xi + i, inner)).start()
            return carry

        lax.fori_loop(0, inner, send_line, 0)

    def send_mate(d, carry):
        head_copy(mate(d)).start()
        return carry

    lax.fori_loop(1, inner, send_mate, 0)

    order = others + [zo]

    def block_wait(ref, send_sem, recv_sem):
        return pltpu.make_async_remote_copy(
            src_ref=ref,
            dst_ref=ref,
            send_sem=send_sem,
            recv_sem=recv_sem,
            device_id={"ep": me},
            device_id_type=MESH,
        )

    for p in others:
        row_copy(p * inner + xi, r_line.at[p], me).wait_recv()
        to_plane(p)

    for name in ("op", "ag", "mg"):
        names[name].wait()
    tile = 512 if width % 512 == 0 else width
    tiles = width // tile
    slices = [slice(t * tile, (t + 1) * tile) for t in range(tiles)]

    def vector(ref, cols):
        return ref[cols].astype(F32).reshape(1, tile)

    def flat(ref, planes, cols):
        parts = []
        for p in planes:
            block = ref[pl.ds(p * inner, inner), :, cols].astype(F32)
            parts.append(block.reshape(plane_rows, block.shape[-1]))
        return parts[0] if len(parts) == 1 else jnp.concatenate(parts, 0)

    def plane_copy(p, d, dst, sem, c):
        return pltpu.make_async_remote_copy(
            src_ref=sbuf.at[p, lax.rem(xi + d, inner)],
            dst_ref=dst.at[p, d],
            send_sem=s_send,
            recv_sem=sem.at[p],
            device_id={"ep": mate(d), "tp": c},
            device_id_type=MESH,
        )

    def plane_send(p, dst, sem, c, first):
        def send(d, carry):
            plane_copy(p, d, dst, sem, c).start()
            return carry

        lax.fori_loop(first, inner, send, 0)

    chunks = len(groups)
    for c in range(chunks):
        group = groups[c]
        rows = group * plane_rows
        planes = order[sum(groups[:c]) : sum(groups[: c + 1])]
        for k, p in enumerate(planes):
            own_plane = c == chunks - 1 and k == group - 1
            count = inner - 1 if own_plane else inner
            block_wait(heads_all.at[pl.ds(0, count)], h_send, h_recv.at[p]).wait_recv()
            block_wait(rows_all.at[pl.ds(0, inner - 1)], r_send, r_plane.at[p]).wait_recv()
        x = flat(heads_all, planes, slice(0, hv)).astype(BF16)
        total = jnp.zeros((rows, 1), F32)
        for cols in slices:
            attn = dot(x, op[:, cols]).astype(BF16).astype(F32)
            value = ALPHA * flat(rows_all, planes, cols) + attn
            wide_rows[:rows, cols] = value
            total = total + row_sum(value)
        center = total / width
        spread = jnp.zeros((rows, 1), F32)
        for cols in slices:
            spread = spread + row_sum(jnp.square(wide_rows[:rows, cols] - center))
        inv = lax.rsqrt(spread / width + EPS)
        gate = jnp.zeros((rows, 1), F32)
        for cols in slices:
            value = (wide_rows[:rows, cols] - center) * inv * vector(attn_gain, cols)
            value = value.astype(BF16)
            mixed[:rows, cols] = value
            if c == chunks - 1:
                own_mixed[:, cols] = value[rows - plane_rows :]
            gate = gate + row_sum(value.astype(F32) * vector(mix_gate, cols))
        blend = 1.0 / (1.0 + jnp.exp(-gate))
        tail = flat(rows_all, planes, slice(width, width + extra))
        c_lane = lax.broadcasted_iota(jnp.int32, (rows, extra), 1)
        weight = row_sum(jnp.where((c_lane == me) | (c_lane == me + n), tail, 0.0))

        if c == 0:
            for name in ("eg", "eu", "ed", "dg", "du", "dd", "og"):
                names[name].wait()
            for w in w_copies:
                w.wait_recv()
        x = mixed[:rows, :]
        for j in range(2):
            value = silu(dot(x, eg[j])) * dot(x, eu[j]) * weight
            hid[:rows, j * half_fe : (j + 1) * half_fe] = value.astype(BF16)
        value = silu(dot(x, dg[...])) * dot(x, du[...]) * blend
        hid[:rows, 2 * half_fe :] = value.astype(BF16)

        for cols in slices:
            part = dot(hid[:rows, :], down[:, cols])
            for k, p in enumerate(planes):
                block = part[k * plane_rows : (k + 1) * plane_rows].reshape(inner, seqs, tile)
                sbuf[p, :, :, cols] = block.astype(BF16)
        for k, p in enumerate(planes):
            if c == chunks - 1 and k == group - 1:
                plane_send(p, rbuf, s_plane, core, 1)
            else:

                @pl.when(core == 1)
                def _():
                    plane_send(p, rbuf, s_plane, core, 1)

                @pl.when(core == 0)
                def _():
                    plane_send(p, obuf, o_plane, other, 0)

    def plane_sum(p, start):
        block_wait(rbuf.at[p, pl.ds(1, inner - 1)], s_send, s_plane.at[p]).wait_recv()

        def one(d, total):
            return total + rbuf[p, d].astype(F32)

        return lax.fori_loop(1, inner, one, start, unroll=inner <= 4)

    def line_send(src, p, c):
        pltpu.make_async_remote_copy(
            src_ref=src.at[p],
            dst_ref=zrecv.at[zo],
            send_sem=s_send,
            recv_sem=s_line,
            device_id={"ep": p * inner + xi, "tp": c},
            device_id_type=MESH,
        ).start()

    @pl.when(core == 1)
    def _():
        for p in others:
            zbuf[p] = plane_sum(p, sbuf[p, xi].astype(F32)).astype(BF16)
            line_send(zbuf, p, core)
            block_wait(obuf.at[p], s_send, o_plane.at[p]).wait_recv()

            def one(d, total):
                return total + obuf[p, d].astype(F32)

            start = obuf[p, 0].astype(F32)
            total = lax.fori_loop(1, inner, one, start, unroll=inner <= 4)
            yout[p] = total.astype(BF16)
            line_send(yout, p, other)

    at = pl.ds(pl.multiple_of(lax.div(xi, 2) * 2 * seqs, 2 * seqs), 2 * seqs)
    pair = own_mixed[at, :]
    pair = pair.astype(F32).reshape(2, seqs, width)
    odd = lax.rem(xi, 2).astype(F32)
    start = ALPHA * (pair[0] + odd * (pair[1] - pair[0]))
    total = plane_sum(zo, start + sbuf[zo, xi].astype(F32))
    if outer > 1:
        block_wait(zrecv.at[pl.ds(0, outer - 1)], s_send, s_line).wait_recv()
    for p in others:
        total = total + zrecv[p].astype(F32)
    center = row_sum(total) / width
    shifted = total - center
    spread = row_sum(jnp.square(shifted)) / width
    gain = out_gain[...].astype(F32).reshape(1, width)
    out[...] = (shifted * lax.rsqrt(spread + EPS) * gain).astype(BF16)

    def sent(ref, sem):
        block_wait(ref, sem, s_line).wait_send()

    sent(heads_all.at[pl.ds(0, n - 1)], h_send)
    sent(rows_all.at[pl.ds(0, n - 1)], r_send)
    sent(rbuf.at[zo, pl.ds(0, inner - 1)], s_send)

    @pl.when(core == 1)
    def _():
        for p in others:
            sent(rbuf.at[p, pl.ds(0, inner - 1)], s_send)
            sent(zrecv.at[pl.ds(0, 2)], s_send)

    @pl.when(core == 0)
    def _():
        for p in others:
            sent(rbuf.at[p], s_send)

    for c in w_copies:
        c.wait_send()


def on_device(
    n,
    residual,
    query_latent,
    query_rotary,
    latent_new,
    rotary_new,
    latent_cache,
    rotary_cache,
    lengths,
    value_up,
    out_proj,
    attn_gain,
    mix_gate,
    dense_w_gate,
    dense_w_up,
    dense_w_down,
    expert_ids,
    expert_scores,
    expert_gate,
    expert_up,
    expert_down,
    out_gain,
):
    seqs, width = residual.shape
    heads = query_latent.shape[1]
    vu = value_up.transpose(1, 2, 0).reshape(-1, value_up.shape[0])
    rotary_turned = rotary_cache.transpose(0, 2, 1)
    extra = -(-2 * n // 128) * 128
    inner = inner_size(n)
    outer = n // inner
    most = max(1, 128 // (inner * seqs))
    groups = [1]
    while sum(groups) < outer:
        groups.append(min(most, outer - sum(groups)))
    top = max(groups) * inner * seqs
    hbm = pl.BlockSpec(memory_space=pl.ANY)
    dma = pltpu.SemaphoreType.DMA
    block = (outer, inner, seqs, width)
    half_fe = expert_gate.shape[-1]
    fd = dense_w_gate.shape[-1]
    return pl.pallas_call(
        functools.partial(kernel, n, tuple(groups)),
        out_shape=pltpu.VMEM((seqs, width), BF16),
        in_specs=[hbm] * 21,
        out_specs=pl.BlockSpec(memory_space=VMEM),
        scratch_shapes=[
            pltpu.SMEM(lengths.shape, jnp.int32),
            VMEM(query_rotary.shape, BF16),
            VMEM(rotary_new.shape, BF16),
            VMEM(query_latent.shape, BF16),
            VMEM(latent_new.shape, BF16),
            VMEM(rotary_turned.shape, BF16),
            VMEM(latent_cache.shape, BF16),
            VMEM(expert_ids.shape, jnp.int32),
            VMEM(expert_scores.shape, F32),
            VMEM(vu.shape, BF16),
            VMEM(out_proj.shape, BF16),
            VMEM(attn_gain.shape, BF16),
            VMEM(mix_gate.shape, BF16),
            VMEM((2,) + expert_gate.shape[1:], BF16),
            VMEM((2,) + expert_up.shape[1:], BF16),
            VMEM((2 * half_fe + fd, width), BF16),
            VMEM(dense_w_gate.shape, BF16),
            VMEM(dense_w_up.shape, BF16),
            VMEM(out_gain.shape, BF16),
            VMEM((seqs * heads, latent_cache.shape[-1]), F32),
            VMEM((n, seqs, width + extra), BF16),
            VMEM((n, seqs, vu.shape[0]), BF16),
            VMEM((top, width), F32),
            VMEM((top, width), BF16),
            VMEM((inner * seqs, width), BF16),
            VMEM((top, 2 * half_fe + fd), BF16),
            VMEM(block, BF16),
            VMEM(block, BF16),
            VMEM((outer, seqs, width), BF16),
            VMEM((outer, seqs, width), BF16),
            dma((20,)),
            dma((seqs,)),
            dma((3,)),
            dma((3,)),
            dma,
            dma((outer,)),
            dma((outer,)),
            dma,
            dma((outer,)),
            dma,
            dma((outer,)),
            dma,
            pltpu.SemaphoreType.REGULAR,
            VMEM(block, BF16),
            VMEM((outer, seqs, width), BF16),
            dma((outer,)),
        ],
        compiler_params=pltpu.CompilerParams(
            collective_id=0, has_side_effects=True, vmem_limit_bytes=60 * 1024 * 1024
        ),
    )(
        lengths,
        query_rotary,
        rotary_new,
        query_latent,
        latent_new,
        rotary_turned,
        latent_cache,
        residual,
        expert_ids,
        expert_scores,
        vu,
        out_proj,
        attn_gain,
        mix_gate,
        expert_gate,
        expert_up,
        expert_down,
        dense_w_gate,
        dense_w_up,
        dense_w_down,
        out_gain,
    )


def solution(mesh):
    rows = P(("ep", "tp"), None)
    rows3 = P(("ep", "tp"), None, None)
    return jax.shard_map(
        functools.partial(on_device, mesh.shape["ep"]),
        mesh=mesh,
        in_specs=(
            rows,
            rows3,
            rows3,
            rows,
            rows,
            rows3,
            rows3,
            P(("ep", "tp")),
            P(),
            P(),
            P(),
            P(),
            P(None, "ep"),
            P(None, "ep"),
            P("ep", None),
            rows,
            rows,
            P("ep", None, "tp"),
            P("ep", None, "tp"),
            P("ep", "tp", None),
            P(),
        ),
        out_specs=rows,
        check_vma=False,
    )
```

```python
import functools
import math

import jax
import jax.numpy as jnp
from jax import lax
from jax.experimental import pallas as pl
from jax.experimental.pallas import tpu as pltpu
from jax.sharding import PartitionSpec as P

NOPE = 64
ALPHA = 8.0**0.25
EPS = 1e-06
ROPE_BASE = 10000.0
F32 = jnp.float32
BF16 = jnp.bfloat16
MESH = pl.DeviceIdType.MESH
VMEM = pltpu.VMEM


def inner_size(n):
    size = 1
    while size * size < n:
        size *= 2
    return size if n % size == 0 else n


def silu(value):
    return value / (1.0 + jnp.exp(-value))


def dot(a, b):
    return jnp.dot(a, b, preferred_element_type=F32)


def dot_nt(a, b):
    return lax.dot_general(a, b, (((1,), (1,)), ((), ())), preferred_element_type=F32)


def row_sum(value):
    return jnp.sum(value, -1, keepdims=True)


def kernel(
    n,
    groups,
    len_hbm,
    qr_hbm,
    rn_hbm,
    ql_hbm,
    ln_hbm,
    rc_hbm,
    cache_hbm,
    res_hbm,
    ids_hbm,
    rs_hbm,
    vu_hbm,
    op_hbm,
    ag_hbm,
    mg_hbm,
    eg_hbm,
    eu_hbm,
    ed_hbm,
    dg_hbm,
    du_hbm,
    dd_hbm,
    og_hbm,
    out,
    lengths,
    query_rotary,
    rotary_new,
    query_latent,
    latent_new,
    rotary_cache,
    cache,
    ids,
    route_scores,
    vu,
    op,
    attn_gain,
    mix_gate,
    eg,
    eu,
    down,
    dg,
    du,
    out_gain,
    lat,
    rows_all,
    heads_all,
    wide_rows,
    mixed,
    own_mixed,
    hid,
    sbuf,
    rbuf,
    zbuf,
    zrecv,
    in_sem,
    cache_sem,
    w_send,
    w_recv,
    r_send,
    r_line,
    r_plane,
    h_send,
    h_recv,
    s_send,
    s_plane,
    s_line,
    ready,
    obuf,
    yout,
    o_plane,
):
    me = lax.axis_index("ep")
    core = lax.axis_index("tp")
    other = 1 - core
    seqs, heads, kl = query_latent.shape
    rope = query_rotary.shape[-1]
    cache_len = cache.shape[1]
    width = res_hbm.shape[1]
    extra = rows_all.shape[-1] - width
    half_fe = eg.shape[-1]
    fd = dg.shape[-1]
    inner = inner_size(n)
    outer = n // inner
    plane_rows = inner * seqs
    zo = lax.div(me, inner)
    xi = lax.rem(me, inner)
    upper = lax.div(2 * zo, outer)

    def descend(k):
        p = outer - 1 - k
        return p - jnp.where(p <= zo, 1, 0)

    def far(k):
        first = descend(k)
        lower = first + lax.min(zo, 1) * ((descend(k - 1) if k else 0) - first)
        return lower + upper * (k + jnp.where(zo <= k, 1, 0) - lower)

    others = [far(k) for k in range(outer - 1)]

    def mate(d):
        return zo * inner + lax.rem(xi + d, inner)

    barrier = pltpu.get_barrier_semaphore()

    def greet(sem, peer):
        pl.semaphore_signal(sem, inc=1, device_id={"ep": peer}, device_id_type=MESH)

    def greet_mate(d, carry):
        greet(barrier, mate(d))
        return carry

    for p in others:
        greet(barrier, p * inner + xi)
    lax.fori_loop(1, inner, greet_mate, 0)
    pl.semaphore_signal(barrier, inc=1, device_id={"tp": other}, device_id_type=MESH)

    own_down = down.at[pl.ds(pl.multiple_of(core * half_fe, half_fe), half_fe)]
    names = {}

    def load(name, a, b):
        c = pltpu.make_async_copy(a, b, in_sem.at[len(names)])
        c.start()
        names[name] = c

    load("len", len_hbm, lengths)
    load("qr", qr_hbm, query_rotary)
    load("rn", rn_hbm, rotary_new)
    load("ql", ql_hbm, query_latent)
    load("ln", ln_hbm, latent_new)
    load("rc", rc_hbm, rotary_cache)
    load("res", res_hbm, rows_all.at[me, :, pl.ds(0, width)])
    load("ids", ids_hbm, ids)
    load("rs", rs_hbm, route_scores)
    cache_copies = [
        pltpu.make_async_copy(cache_hbm.at[s], cache.at[s], cache_sem) for s in range(seqs)
    ]
    for c in cache_copies:
        c.start()

    half = rope // 2
    names["len"].wait()
    lane = lax.broadcasted_iota(jnp.int32, (seqs, rope), 1)
    row = lax.broadcasted_iota(jnp.int32, (seqs, rope), 0)
    pos = jnp.zeros((seqs, rope), F32)
    for s in range(seqs):
        pos = jnp.where(row == s, lengths[s].astype(F32), pos)
    inv_freq = jnp.exp(lax.rem(lane, half).astype(F32) * (-math.log(ROPE_BASE) / half))
    angles = pos * inv_freq
    cosine = jnp.cos(angles)
    sine = jnp.sin(angles)
    ra = lax.broadcasted_iota(jnp.int32, (rope, rope), 0)
    rb = lax.broadcasted_iota(jnp.int32, (rope, rope), 1)
    swap = jnp.where(ra + half == rb, 1.0, jnp.where(ra == rb + half, -1.0, 0.0)).astype(BF16)
    for name in ("qr", "rn", "ql", "ln", "rc"):
        names[name].wait()
    q_rot = query_rotary[...].astype(F32).reshape(seqs * heads, rope)
    q_swap = dot(q_rot.astype(BF16), swap).reshape(seqs, heads, rope)
    q_rot = q_rot.reshape(seqs, heads, rope)
    k_rot = rotary_new[...]
    k_turn = (k_rot.astype(F32) * cosine + dot(k_rot, swap) * sine).astype(BF16).astype(F32)
    ln_all = latent_new[...].astype(F32)
    score_scale = (NOPE + rope) ** (-0.5)
    t_idx = lax.broadcasted_iota(jnp.int32, (heads, cache_len), 1)

    names["ids"].wait()
    names["rs"].wait()
    sc = route_scores[...]
    share = sc / row_sum(sc)
    e_lane = lax.broadcasted_iota(jnp.int32, (seqs, extra), 1)
    low = e_lane >= n
    e_idx = jnp.where(low, e_lane - n, e_lane)
    coef = jnp.zeros((seqs, extra), F32)
    for k in range(ids.shape[1]):
        coef = coef + jnp.where(e_idx == ids[:, k : k + 1], share[:, k : k + 1], 0.0)
    high = coef.astype(BF16)
    coef = jnp.where(low, coef - high.astype(F32), high.astype(F32)).astype(BF16)
    rows_all[me, :, width:] = coef

    def row_copy(block, sem, target):
        return pltpu.make_async_remote_copy(
            src_ref=rows_all.at[block],
            dst_ref=rows_all.at[block],
            send_sem=r_send,
            recv_sem=sem,
            device_id={"ep": target},
            device_id_type=MESH,
        )

    def to_plane(p):
        block = p * inner + xi

        def send(d, carry):
            row_copy(block, r_plane.at[p], mate(d)).start()
            return carry

        lax.fori_loop(1, inner, send, 0)

    pairs = [(eg_hbm.at[0], eg.at[core]), (eu_hbm.at[0], eu.at[core]), (ed_hbm.at[0], own_down)]
    w_copies = [
        pltpu.make_async_remote_copy(
            src_ref=a,
            dst_ref=b,
            send_sem=w_send.at[k],
            recv_sem=w_recv.at[k],
            device_id={"tp": other},
            device_id_type=MESH,
        )
        for k, (a, b) in enumerate(pairs)
    ]
    def announce():
        pl.semaphore_wait(barrier, outer + inner - 1)
        for p in others:
            greet(ready, p * inner + xi)

        for p in others:
            row_copy(me, r_line.at[zo], p * inner + xi).start()
        to_plane(zo)
        for c in w_copies:
            c.start()

    names["res"].wait()
    @pl.when(upper == 1)
    def _():
        announce()

    score_rows, own_rows_all = [], []
    for s in range(seqs):
        q_turn = (q_rot[s] * cosine[s : s + 1] + q_swap[s] * sine[s : s + 1]).astype(BF16)
        ql = query_latent[s]
        own_rows_all.append(
            row_sum(ql.astype(F32) * ln_all[s : s + 1])
            + row_sum(q_turn.astype(F32) * k_turn[s : s + 1])
        )
        rot_part = dot(q_turn, rotary_cache[s])
        if s == 0:
            pltpu.make_async_copy(cache_hbm, cache, cache_sem).wait()
        part = dot_nt(ql, cache[s]) + rot_part
        score_rows.append(jnp.where(t_idx < lengths[s], part, -jnp.inf))
    load("vu", vu_hbm, vu)
    load("op", op_hbm, op)
    load("ag", ag_hbm, attn_gain)
    load("mg", mg_hbm, mix_gate)
    load("eg", eg_hbm.at[0], eg.at[core])
    pltpu.make_async_copy(eu_hbm.at[0], eu.at[core], in_sem.at[len(names) - 1]).start()
    names["eg"] = pltpu.make_async_copy(eg, eg, in_sem.at[len(names) - 1])
    sum_ed = len(names)
    load("ed", ed_hbm.at[0], own_down)
    both = down.at[pl.ds(0, half_fe + fd)]
    names["ed"] = pltpu.make_async_copy(both, both, in_sem.at[sum_ed])
    load("dg", dg_hbm, dg)
    load("du", du_hbm, du)
    pltpu.make_async_copy(dd_hbm, down.at[pl.ds(2 * half_fe, fd)], in_sem.at[sum_ed]).start()
    load("og", og_hbm, out_gain)
    own = jnp.concatenate(own_rows_all, 0) * score_scale
    scores = jnp.concatenate(score_rows, 0) * score_scale

    @pl.when(upper == 0)
    def _():
        announce()

    top = jnp.maximum(jnp.max(scores, -1, keepdims=True), own)
    probs = jnp.exp(scores - top)
    own_p = jnp.exp(own - top)
    total = row_sum(probs) + own_p
    weights = probs / total
    own_w = (own_p / total).astype(BF16).astype(F32)
    for s in range(seqs):
        at = slice(s * heads, (s + 1) * heads)
        lat[at, :] = dot(weights[at].astype(BF16), cache[s]) + own_w[at] * ln_all[s : s + 1]

    names["vu"].wait()
    wide = dot_nt(lat[...].astype(BF16), vu[...])
    hv = wide.shape[1]
    vdim = hv // heads
    wide = wide.reshape(seqs, heads, hv)
    h_row = lax.broadcasted_iota(jnp.int32, wide.shape, 1)
    h_lane = lax.broadcasted_iota(jnp.int32, wide.shape, 2)
    own_head = (h_lane >= h_row * vdim) & (h_lane < (h_row + 1) * vdim)
    heads_all[me] = jnp.sum(jnp.where(own_head, wide, 0.0), 1).astype(BF16)

    if outer > 1:
        pl.semaphore_wait(ready, outer - 1)

    def head_copy(target):
        return pltpu.make_async_remote_copy(
            src_ref=heads_all.at[me],
            dst_ref=heads_all.at[me],
            send_sem=h_send,
            recv_sem=h_recv.at[zo],
            device_id={"ep": target},
            device_id_type=MESH,
        )

    for p in others:

        def send_line(i, carry):
            head_copy(p * inner + lax.rem(xi + i, inner)).start()
            return carry

        lax.fori_loop(0, inner, send_line, 0)

    def send_mate(d, carry):
        head_copy(mate(d)).start()
        return carry

    lax.fori_loop(1, inner, send_mate, 0)

    order = [zo] + others

    def block_wait(ref, send_sem, recv_sem):
        return pltpu.make_async_remote_copy(
            src_ref=ref,
            dst_ref=ref,
            send_sem=send_sem,
            recv_sem=recv_sem,
            device_id={"ep": me},
            device_id_type=MESH,
        )

    for p in others:
        row_copy(p * inner + xi, r_line.at[p], me).wait_recv()
        to_plane(p)

    for name in ("op", "ag", "mg"):
        names[name].wait()
    tile = 512 if width % 512 == 0 else width
    tiles = width // tile
    slices = [slice(t * tile, (t + 1) * tile) for t in range(tiles)]

    def vector(ref, cols):
        return ref[cols].astype(F32).reshape(1, tile)

    def flat(ref, planes, cols):
        parts = []
        for p in planes:
            block = ref[pl.ds(p * inner, inner), :, cols].astype(F32)
            parts.append(block.reshape(plane_rows, block.shape[-1]))
        return parts[0] if len(parts) == 1 else jnp.concatenate(parts, 0)

    def plane_copy(p, d, dst, sem, c):
        return pltpu.make_async_remote_copy(
            src_ref=sbuf.at[p, lax.rem(xi + d, inner)],
            dst_ref=dst.at[p, d],
            send_sem=s_send,
            recv_sem=sem.at[p],
            device_id={"ep": mate(d), "tp": c},
            device_id_type=MESH,
        )

    def plane_send(p, dst, sem, c, first):
        def send(d, carry):
            plane_copy(p, d, dst, sem, c).start()
            return carry

        lax.fori_loop(first, inner, send, 0)

    chunks = len(groups)
    for c in range(chunks):
        group = groups[c]
        rows = group * plane_rows
        planes = order[sum(groups[:c]) : sum(groups[: c + 1])]
        for k, p in enumerate(planes):
            own_plane = c == 0 and k == group - 1
            count = inner - 1 if own_plane else inner
            block_wait(heads_all.at[pl.ds(0, count)], h_send, h_recv.at[p]).wait_recv()
            block_wait(rows_all.at[pl.ds(0, inner - 1)], r_send, r_plane.at[p]).wait_recv()
        x = flat(heads_all, planes, slice(0, hv)).astype(BF16)
        total = jnp.zeros((rows, 1), F32)
        for cols in slices:
            attn = dot(x, op[:, cols]).astype(BF16).astype(F32)
            value = ALPHA * flat(rows_all, planes, cols) + attn
            wide_rows[:rows, cols] = value
            total = total + row_sum(value)
        center = total / width
        spread = jnp.zeros((rows, 1), F32)
        for cols in slices:
            spread = spread + row_sum(jnp.square(wide_rows[:rows, cols] - center))
        inv = lax.rsqrt(spread / width + EPS)
        gate = jnp.zeros((rows, 1), F32)
        for cols in slices:
            value = (wide_rows[:rows, cols] - center) * inv * vector(attn_gain, cols)
            value = value.astype(BF16)
            mixed[:rows, cols] = value
            if c == 0:
                own_mixed[:, cols] = value[rows - plane_rows :]
            gate = gate + row_sum(value.astype(F32) * vector(mix_gate, cols))
        blend = 1.0 / (1.0 + jnp.exp(-gate))
        tail = flat(rows_all, planes, slice(width, width + extra))
        c_lane = lax.broadcasted_iota(jnp.int32, (rows, extra), 1)
        weight = row_sum(jnp.where((c_lane == me) | (c_lane == me + n), tail, 0.0))

        if c == 0:
            for name in ("eg", "ed", "dg", "du", "og"):
                names[name].wait()
            for w in w_copies:
                w.wait_recv()
        x = mixed[:rows, :]
        for j in range(2):
            value = silu(dot(x, eg[j])) * dot(x, eu[j]) * weight
            hid[:rows, j * half_fe : (j + 1) * half_fe] = value.astype(BF16)
        value = silu(dot(x, dg[...])) * dot(x, du[...]) * blend
        hid[:rows, 2 * half_fe :] = value.astype(BF16)

        for cols in slices:
            part = dot(hid[:rows, :], down[:, cols])
            for k, p in enumerate(planes):
                block = part[k * plane_rows : (k + 1) * plane_rows].reshape(inner, seqs, tile)
                sbuf[p, :, :, cols] = block.astype(BF16)
        for k, p in enumerate(planes):
            if c == 0 and k == group - 1:
                plane_send(p, rbuf, s_plane, core, 1)
            else:

                @pl.when(core == 1)
                def _():
                    plane_send(p, rbuf, s_plane, core, 1)

                @pl.when(core == 0)
                def _():
                    plane_send(p, obuf, o_plane, other, 0)

    def plane_sum(p, start):
        block_wait(rbuf.at[p, pl.ds(1, inner - 1)], s_send, s_plane.at[p]).wait_recv()

        def one(d, total):
            return total + rbuf[p, d].astype(F32)

        return lax.fori_loop(1, inner, one, start, unroll=inner <= 4)

    def line_send(src, p, c):
        pltpu.make_async_remote_copy(
            src_ref=src.at[p],
            dst_ref=zrecv.at[zo],
            send_sem=s_send,
            recv_sem=s_line,
            device_id={"ep": p * inner + xi, "tp": c},
            device_id_type=MESH,
        ).start()

    @pl.when(core == 1)
    def _():
        for p in others:
            zbuf[p] = plane_sum(p, sbuf[p, xi].astype(F32)).astype(BF16)
            line_send(zbuf, p, core)
            block_wait(obuf.at[p], s_send, o_plane.at[p]).wait_recv()

            def one(d, total):
                return total + obuf[p, d].astype(F32)

            start = obuf[p, 0].astype(F32)
            total = lax.fori_loop(1, inner, one, start, unroll=inner <= 4)
            yout[p] = total.astype(BF16)
            line_send(yout, p, other)

    at = pl.ds(pl.multiple_of(lax.div(xi, 2) * 2 * seqs, 2 * seqs), 2 * seqs)
    pair = own_mixed[at, :]
    pair = pair.astype(F32).reshape(2, seqs, width)
    odd = lax.rem(xi, 2).astype(F32)
    start = ALPHA * (pair[0] + odd * (pair[1] - pair[0]))
    total = plane_sum(zo, start + sbuf[zo, xi].astype(F32))
    if outer > 1:
        block_wait(zrecv.at[pl.ds(0, outer - 1)], s_send, s_line).wait_recv()
    for p in others:
        total = total + zrecv[p].astype(F32)
    center = row_sum(total) / width
    shifted = total - center
    spread = row_sum(jnp.square(shifted)) / width
    gain = out_gain[...].astype(F32).reshape(1, width)
    out[...] = (shifted * lax.rsqrt(spread + EPS) * gain).astype(BF16)

    def sent(ref, sem):
        block_wait(ref, sem, s_line).wait_send()

    sent(heads_all.at[pl.ds(0, n - 1)], h_send)
    sent(rows_all.at[pl.ds(0, n - 1)], r_send)
    sent(rbuf.at[zo, pl.ds(0, inner - 1)], s_send)

    @pl.when(core == 1)
    def _():
        for p in others:
            sent(rbuf.at[p, pl.ds(0, inner - 1)], s_send)
            sent(zrecv.at[pl.ds(0, 2)], s_send)

    @pl.when(core == 0)
    def _():
        for p in others:
            sent(rbuf.at[p], s_send)

    for c in w_copies:
        c.wait_send()


def on_device(
    n,
    residual,
    query_latent,
    query_rotary,
    latent_new,
    rotary_new,
    latent_cache,
    rotary_cache,
    lengths,
    value_up,
    out_proj,
    attn_gain,
    mix_gate,
    dense_w_gate,
    dense_w_up,
    dense_w_down,
    expert_ids,
    expert_scores,
    expert_gate,
    expert_up,
    expert_down,
    out_gain,
):
    seqs, width = residual.shape
    heads = query_latent.shape[1]
    vu = value_up.transpose(1, 2, 0).reshape(-1, value_up.shape[0])
    rotary_turned = rotary_cache.transpose(0, 2, 1)
    extra = -(-2 * n // 128) * 128
    inner = inner_size(n)
    outer = n // inner
    most = max(1, 128 // (inner * seqs))
    groups = [1] * min(outer, 2)
    while sum(groups) < outer:
        groups.append(min(most, outer - sum(groups)))
    top = max(groups) * inner * seqs
    hbm = pl.BlockSpec(memory_space=pl.ANY)
    dma = pltpu.SemaphoreType.DMA
    block = (outer, inner, seqs, width)
    half_fe = expert_gate.shape[-1]
    fd = dense_w_gate.shape[-1]
    return pl.pallas_call(
        functools.partial(kernel, n, tuple(groups)),
        out_shape=pltpu.VMEM((seqs, width), BF16),
        in_specs=[hbm] * 21,
        out_specs=pl.BlockSpec(memory_space=VMEM),
        scratch_shapes=[
            pltpu.SMEM(lengths.shape, jnp.int32),
            VMEM(query_rotary.shape, BF16),
            VMEM(rotary_new.shape, BF16),
            VMEM(query_latent.shape, BF16),
            VMEM(latent_new.shape, BF16),
            VMEM(rotary_turned.shape, BF16),
            VMEM(latent_cache.shape, BF16),
            VMEM(expert_ids.shape, jnp.int32),
            VMEM(expert_scores.shape, F32),
            VMEM(vu.shape, BF16),
            VMEM(out_proj.shape, BF16),
            VMEM(attn_gain.shape, BF16),
            VMEM(mix_gate.shape, BF16),
            VMEM((2,) + expert_gate.shape[1:], BF16),
            VMEM((2,) + expert_up.shape[1:], BF16),
            VMEM((2 * half_fe + fd, width), BF16),
            VMEM(dense_w_gate.shape, BF16),
            VMEM(dense_w_up.shape, BF16),
            VMEM(out_gain.shape, BF16),
            VMEM((seqs * heads, latent_cache.shape[-1]), F32),
            VMEM((n, seqs, width + extra), BF16),
            VMEM((n, seqs, vu.shape[0]), BF16),
            VMEM((top, width), F32),
            VMEM((top, width), BF16),
            VMEM((inner * seqs, width), BF16),
            VMEM((top, 2 * half_fe + fd), BF16),
            VMEM(block, BF16),
            VMEM(block, BF16),
            VMEM((outer, seqs, width), BF16),
            VMEM((outer, seqs, width), BF16),
            dma((18,)),
            dma,
            dma((3,)),
            dma((3,)),
            dma,
            dma((outer,)),
            dma((outer,)),
            dma,
            dma((outer,)),
            dma,
            dma((outer,)),
            dma,
            pltpu.SemaphoreType.REGULAR,
            VMEM(block, BF16),
            VMEM((outer, seqs, width), BF16),
            dma((outer,)),
        ],
        compiler_params=pltpu.CompilerParams(
            collective_id=0, has_side_effects=True, vmem_limit_bytes=60 * 1024 * 1024
        ),
    )(
        lengths,
        query_rotary,
        rotary_new,
        query_latent,
        latent_new,
        rotary_turned,
        latent_cache,
        residual,
        expert_ids,
        expert_scores,
        vu,
        out_proj,
        attn_gain,
        mix_gate,
        expert_gate,
        expert_up,
        expert_down,
        dense_w_gate,
        dense_w_up,
        dense_w_down,
        out_gain,
    )


def solution(mesh):
    rows = P(("ep", "tp"), None)
    rows3 = P(("ep", "tp"), None, None)
    return jax.shard_map(
        functools.partial(on_device, mesh.shape["ep"]),
        mesh=mesh,
        in_specs=(
            rows,
            rows3,
            rows3,
            rows,
            rows,
            rows3,
            rows3,
            P(("ep", "tp")),
            P(),
            P(),
            P(),
            P(),
            P(None, "ep"),
            P(None, "ep"),
            P("ep", None),
            rows,
            rows,
            P("ep", None, "tp"),
            P("ep", None, "tp"),
            P("ep", "tp", None),
            P(),
        ),
        out_specs=rows,
        check_vma=False,
    )
```

```python
import functools
import math

import jax
import jax.numpy as jnp
from jax import lax
from jax.experimental import pallas as pl
from jax.experimental.pallas import tpu as pltpu
from jax.sharding import PartitionSpec as P

NOPE = 64
ALPHA = 8.0**0.25
EPS = 1e-06
ROPE_BASE = 10000.0
F32 = jnp.float32
BF16 = jnp.bfloat16
MESH = pl.DeviceIdType.MESH
VMEM = pltpu.VMEM


def inner_size(n):
    size = 1
    while size * size < n:
        size *= 2
    return size if n % size == 0 else n


def silu(value):
    return value / (1.0 + jnp.exp(-value))


def dot(a, b):
    return jnp.dot(a, b, preferred_element_type=F32)


def dot_nt(a, b):
    return lax.dot_general(a, b, (((1,), (1,)), ((), ())), preferred_element_type=F32)


def row_sum(value):
    return jnp.sum(value, -1, keepdims=True)


def kernel(
    n,
    groups,
    len_hbm,
    qr_hbm,
    rn_hbm,
    ql_hbm,
    ln_hbm,
    rc_hbm,
    cache_hbm,
    res_hbm,
    ids_hbm,
    rs_hbm,
    vu_hbm,
    op_hbm,
    ag_hbm,
    mg_hbm,
    eg_hbm,
    eu_hbm,
    ed_hbm,
    dg_hbm,
    du_hbm,
    dd_hbm,
    og_hbm,
    out,
    lengths,
    query_rotary,
    rotary_new,
    query_latent,
    latent_new,
    rotary_cache,
    cache,
    ids,
    route_scores,
    vu,
    op,
    attn_gain,
    mix_gate,
    eg,
    eu,
    down,
    dg,
    du,
    out_gain,
    lat,
    rows_all,
    heads_all,
    wide_rows,
    mixed,
    own_mixed,
    hid,
    sbuf,
    rbuf,
    zbuf,
    zrecv,
    in_sem,
    cache_sem,
    w_send,
    w_recv,
    r_send,
    r_line,
    r_plane,
    h_send,
    h_recv,
    s_send,
    s_plane,
    s_line,
    ready,
    obuf,
    yout,
    o_plane,
):
    me = lax.axis_index("ep")
    core = lax.axis_index("tp")
    other = 1 - core
    seqs, heads, kl = query_latent.shape
    rope = query_rotary.shape[-1]
    cache_len = cache.shape[1]
    width = res_hbm.shape[1]
    extra = rows_all.shape[-1] - width
    half_fe = eg.shape[-1]
    fd = dg.shape[-1]
    inner = inner_size(n)
    outer = n // inner
    plane_rows = inner * seqs
    zo = lax.div(me, inner)
    xi = lax.rem(me, inner)
    upper = lax.div(2 * zo, outer)

    def descend(k):
        p = outer - 1 - k
        return p - jnp.where(p <= zo, 1, 0)

    def far(k):
        first = descend(k)
        lower = first + lax.min(zo, 1) * ((descend(k - 1) if k else 0) - first)
        return lower + upper * (k + jnp.where(zo <= k, 1, 0) - lower)

    others = [far(k) for k in range(outer - 1)]

    def mate(d):
        return zo * inner + lax.rem(xi + d, inner)

    barrier = pltpu.get_barrier_semaphore()

    def greet(sem, peer):
        pl.semaphore_signal(sem, inc=1, device_id={"ep": peer}, device_id_type=MESH)

    def greet_mate(d, carry):
        greet(barrier, mate(d))
        return carry

    for p in others:
        greet(barrier, p * inner + xi)
    lax.fori_loop(1, inner, greet_mate, 0)
    pl.semaphore_signal(barrier, inc=1, device_id={"tp": other}, device_id_type=MESH)

    own_down = down.at[pl.ds(pl.multiple_of(core * half_fe, half_fe), half_fe)]
    names = {}

    def load(name, a, b):
        c = pltpu.make_async_copy(a, b, in_sem.at[len(names)])
        c.start()
        names[name] = c

    load("len", len_hbm, lengths)
    load("qr", qr_hbm, query_rotary)
    load("rn", rn_hbm, rotary_new)
    load("ql", ql_hbm, query_latent)
    load("ln", ln_hbm, latent_new)
    load("rc", rc_hbm, rotary_cache)
    load("res", res_hbm, rows_all.at[me, :, pl.ds(0, width)])
    load("ids", ids_hbm, ids)
    load("rs", rs_hbm, route_scores)
    cache_copies = [
        pltpu.make_async_copy(cache_hbm.at[s], cache.at[s], cache_sem) for s in range(seqs)
    ]
    for c in cache_copies:
        c.start()

    half = rope // 2
    names["len"].wait()
    lane = lax.broadcasted_iota(jnp.int32, (seqs, rope), 1)
    row = lax.broadcasted_iota(jnp.int32, (seqs, rope), 0)
    pos = jnp.zeros((seqs, rope), F32)
    for s in range(seqs):
        pos = jnp.where(row == s, lengths[s].astype(F32), pos)
    inv_freq = jnp.exp(lax.rem(lane, half).astype(F32) * (-math.log(ROPE_BASE) / half))
    angles = pos * inv_freq
    cosine = jnp.cos(angles)
    sine = jnp.sin(angles)
    ra = lax.broadcasted_iota(jnp.int32, (rope, rope), 0)
    rb = lax.broadcasted_iota(jnp.int32, (rope, rope), 1)
    swap = jnp.where(ra + half == rb, 1.0, jnp.where(ra == rb + half, -1.0, 0.0)).astype(BF16)
    for name in ("qr", "rn", "ql", "ln", "rc"):
        names[name].wait()
    q_rot = query_rotary[...].astype(F32).reshape(seqs * heads, rope)
    q_swap = dot(q_rot.astype(BF16), swap).reshape(seqs, heads, rope)
    q_rot = q_rot.reshape(seqs, heads, rope)
    k_rot = rotary_new[...]
    k_turn = (k_rot.astype(F32) * cosine + dot(k_rot, swap) * sine).astype(BF16).astype(F32)
    ln_all = latent_new[...].astype(F32)
    score_scale = (NOPE + rope) ** (-0.5)
    t_idx = lax.broadcasted_iota(jnp.int32, (heads, cache_len), 1)

    names["ids"].wait()
    names["rs"].wait()
    sc = route_scores[...]
    share = sc / row_sum(sc)
    e_lane = lax.broadcasted_iota(jnp.int32, (seqs, extra), 1)
    low = e_lane >= n
    e_idx = jnp.where(low, e_lane - n, e_lane)
    coef = jnp.zeros((seqs, extra), F32)
    for k in range(ids.shape[1]):
        coef = coef + jnp.where(e_idx == ids[:, k : k + 1], share[:, k : k + 1], 0.0)
    high = coef.astype(BF16)
    coef = jnp.where(low, coef - high.astype(F32), high.astype(F32)).astype(BF16)
    rows_all[me, :, width:] = coef

    def row_copy(block, sem, target):
        return pltpu.make_async_remote_copy(
            src_ref=rows_all.at[block],
            dst_ref=rows_all.at[block],
            send_sem=r_send,
            recv_sem=sem,
            device_id={"ep": target},
            device_id_type=MESH,
        )

    def to_plane(p):
        block = p * inner + xi

        def send(d, carry):
            row_copy(block, r_plane.at[p], mate(d)).start()
            return carry

        lax.fori_loop(1, inner, send, 0)

    pairs = [(eg_hbm.at[0], eg.at[core]), (eu_hbm.at[0], eu.at[core]), (ed_hbm.at[0], own_down)]
    w_copies = [
        pltpu.make_async_remote_copy(
            src_ref=a,
            dst_ref=b,
            send_sem=w_send.at[k],
            recv_sem=w_recv.at[k],
            device_id={"tp": other},
            device_id_type=MESH,
        )
        for k, (a, b) in enumerate(pairs)
    ]
    def announce():
        pl.semaphore_wait(barrier, outer + inner - 1)
        for p in others:
            greet(ready, p * inner + xi)

        for p in others:
            row_copy(me, r_line.at[zo], p * inner + xi).start()
        to_plane(zo)
        for c in w_copies:
            c.start()

    names["res"].wait()
    @pl.when(upper == 1)
    def _():
        announce()

    score_rows, own_rows_all = [], []
    for s in range(seqs):
        q_turn = (q_rot[s] * cosine[s : s + 1] + q_swap[s] * sine[s : s + 1]).astype(BF16)
        ql = query_latent[s]
        own_rows_all.append(
            row_sum(ql.astype(F32) * ln_all[s : s + 1])
            + row_sum(q_turn.astype(F32) * k_turn[s : s + 1])
        )
        rot_part = dot(q_turn, rotary_cache[s])
        if s == 0:
            pltpu.make_async_copy(cache_hbm, cache, cache_sem).wait()
        part = dot_nt(ql, cache[s]) + rot_part
        score_rows.append(jnp.where(t_idx < lengths[s], part, -jnp.inf))
    load("vu", vu_hbm, vu)
    load("op", op_hbm, op)
    load("ag", ag_hbm, attn_gain)
    load("mg", mg_hbm, mix_gate)
    load("eg", eg_hbm.at[0], eg.at[core])
    pltpu.make_async_copy(eu_hbm.at[0], eu.at[core], in_sem.at[len(names) - 1]).start()
    names["eg"] = pltpu.make_async_copy(eg, eg, in_sem.at[len(names) - 1])
    sum_ed = len(names)
    load("ed", ed_hbm.at[0], own_down)
    both = down.at[pl.ds(0, half_fe + fd)]
    names["ed"] = pltpu.make_async_copy(both, both, in_sem.at[sum_ed])
    load("dg", dg_hbm, dg)
    load("du", du_hbm, du)
    pltpu.make_async_copy(dd_hbm, down.at[pl.ds(2 * half_fe, fd)], in_sem.at[sum_ed]).start()
    load("og", og_hbm, out_gain)
    own = jnp.concatenate(own_rows_all, 0) * score_scale
    scores = jnp.concatenate(score_rows, 0) * score_scale

    @pl.when(upper == 0)
    def _():
        announce()

    top = jnp.maximum(jnp.max(scores, -1, keepdims=True), own)
    probs = jnp.exp(scores - top)
    own_p = jnp.exp(own - top)
    total = row_sum(probs) + own_p
    weights = probs / total
    own_w = (own_p / total).astype(BF16).astype(F32)
    for s in range(seqs):
        at = slice(s * heads, (s + 1) * heads)
        lat[at, :] = dot(weights[at].astype(BF16), cache[s]) + own_w[at] * ln_all[s : s + 1]

    names["vu"].wait()
    wide = dot_nt(lat[...].astype(BF16), vu[...])
    hv = wide.shape[1]
    vdim = hv // heads
    wide = wide.reshape(seqs, heads, hv)
    h_row = lax.broadcasted_iota(jnp.int32, wide.shape, 1)
    h_lane = lax.broadcasted_iota(jnp.int32, wide.shape, 2)
    own_head = (h_lane >= h_row * vdim) & (h_lane < (h_row + 1) * vdim)
    heads_all[me] = jnp.sum(jnp.where(own_head, wide, 0.0), 1).astype(BF16)

    if outer > 1:
        pl.semaphore_wait(ready, outer - 1)

    def head_copy(target):
        return pltpu.make_async_remote_copy(
            src_ref=heads_all.at[me],
            dst_ref=heads_all.at[me],
            send_sem=h_send,
            recv_sem=h_recv.at[zo],
            device_id={"ep": target},
            device_id_type=MESH,
        )

    def send_mate(d, carry):
        head_copy(mate(d)).start()
        return carry

    lax.fori_loop(1, inner, send_mate, 0)

    for p in others:

        def send_line(i, carry):
            head_copy(p * inner + lax.rem(xi + i, inner)).start()
            return carry

        lax.fori_loop(0, inner, send_line, 0)


    order = [zo] + others

    def block_wait(ref, send_sem, recv_sem):
        return pltpu.make_async_remote_copy(
            src_ref=ref,
            dst_ref=ref,
            send_sem=send_sem,
            recv_sem=recv_sem,
            device_id={"ep": me},
            device_id_type=MESH,
        )

    for p in others:
        row_copy(p * inner + xi, r_line.at[p], me).wait_recv()
        to_plane(p)

    for name in ("op", "ag", "mg"):
        names[name].wait()
    tile = 512 if width % 512 == 0 else width
    tiles = width // tile
    slices = [slice(t * tile, (t + 1) * tile) for t in range(tiles)]

    def vector(ref, cols):
        return ref[cols].astype(F32).reshape(1, tile)

    def flat(ref, planes, cols):
        parts = []
        for p in planes:
            block = ref[pl.ds(p * inner, inner), :, cols].astype(F32)
            parts.append(block.reshape(plane_rows, block.shape[-1]))
        return parts[0] if len(parts) == 1 else jnp.concatenate(parts, 0)

    def plane_copy(p, d, dst, sem, c):
        return pltpu.make_async_remote_copy(
            src_ref=sbuf.at[p, lax.rem(xi + d, inner)],
            dst_ref=dst.at[p, d],
            send_sem=s_send,
            recv_sem=sem.at[p],
            device_id={"ep": mate(d), "tp": c},
            device_id_type=MESH,
        )

    def plane_send(p, dst, sem, c, first):
        def send(d, carry):
            plane_copy(p, d, dst, sem, c).start()
            return carry

        lax.fori_loop(first, inner, send, 0)

    chunks = len(groups)
    for c in range(chunks):
        group = groups[c]
        rows = group * plane_rows
        planes = order[sum(groups[:c]) : sum(groups[: c + 1])]
        for k, p in enumerate(planes):
            own_plane = c == 0 and k == group - 1
            count = inner - 1 if own_plane else inner
            block_wait(heads_all.at[pl.ds(0, count)], h_send, h_recv.at[p]).wait_recv()
            block_wait(rows_all.at[pl.ds(0, inner - 1)], r_send, r_plane.at[p]).wait_recv()
        x = flat(heads_all, planes, slice(0, hv)).astype(BF16)
        total = jnp.zeros((rows, 1), F32)
        for cols in slices:
            attn = dot(x, op[:, cols]).astype(BF16).astype(F32)
            value = ALPHA * flat(rows_all, planes, cols) + attn
            wide_rows[:rows, cols] = value
            total = total + row_sum(value)
        center = total / width
        spread = jnp.zeros((rows, 1), F32)
        for cols in slices:
            spread = spread + row_sum(jnp.square(wide_rows[:rows, cols] - center))
        inv = lax.rsqrt(spread / width + EPS)
        gate = jnp.zeros((rows, 1), F32)
        for cols in slices:
            value = (wide_rows[:rows, cols] - center) * inv * vector(attn_gain, cols)
            value = value.astype(BF16)
            mixed[:rows, cols] = value
            if c == 0:
                own_mixed[:, cols] = value[rows - plane_rows :]
            gate = gate + row_sum(value.astype(F32) * vector(mix_gate, cols))
        blend = 1.0 / (1.0 + jnp.exp(-gate))
        tail = flat(rows_all, planes, slice(width, width + extra))
        c_lane = lax.broadcasted_iota(jnp.int32, (rows, extra), 1)
        weight = row_sum(jnp.where((c_lane == me) | (c_lane == me + n), tail, 0.0))

        if c == 0:
            for name in ("eg", "ed", "dg", "du", "og"):
                names[name].wait()
            for w in w_copies:
                w.wait_recv()
        x = mixed[:rows, :]
        for j in range(2):
            value = silu(dot(x, eg[j])) * dot(x, eu[j]) * weight
            hid[:rows, j * half_fe : (j + 1) * half_fe] = value.astype(BF16)
        value = silu(dot(x, dg[...])) * dot(x, du[...]) * blend
        hid[:rows, 2 * half_fe :] = value.astype(BF16)

        for cols in slices:
            part = dot(hid[:rows, :], down[:, cols])
            for k, p in enumerate(planes):
                block = part[k * plane_rows : (k + 1) * plane_rows].reshape(inner, seqs, tile)
                sbuf[p, :, :, cols] = block.astype(BF16)
        for k, p in enumerate(planes):
            if c == 0 and k == group - 1:
                plane_send(p, rbuf, s_plane, core, 1)
            else:

                @pl.when(core == 1)
                def _():
                    plane_send(p, rbuf, s_plane, core, 1)

                @pl.when(core == 0)
                def _():
                    plane_send(p, obuf, o_plane, other, 0)

    def plane_sum(p, start):
        block_wait(rbuf.at[p, pl.ds(1, inner - 1)], s_send, s_plane.at[p]).wait_recv()

        def one(d, total):
            return total + rbuf[p, d].astype(F32)

        return lax.fori_loop(1, inner, one, start, unroll=inner <= 4)

    def line_send(src, p, c):
        pltpu.make_async_remote_copy(
            src_ref=src.at[p],
            dst_ref=zrecv.at[zo],
            send_sem=s_send,
            recv_sem=s_line,
            device_id={"ep": p * inner + xi, "tp": c},
            device_id_type=MESH,
        ).start()

    @pl.when(core == 1)
    def _():
        for p in others:
            zbuf[p] = plane_sum(p, sbuf[p, xi].astype(F32)).astype(BF16)
            line_send(zbuf, p, core)
            block_wait(obuf.at[p], s_send, o_plane.at[p]).wait_recv()

            def one(d, total):
                return total + obuf[p, d].astype(F32)

            start = obuf[p, 0].astype(F32)
            total = lax.fori_loop(1, inner, one, start, unroll=inner <= 4)
            yout[p] = total.astype(BF16)
            line_send(yout, p, other)

    at = pl.ds(pl.multiple_of(lax.div(xi, 2) * 2 * seqs, 2 * seqs), 2 * seqs)
    pair = own_mixed[at, :]
    pair = pair.astype(F32).reshape(2, seqs, width)
    odd = lax.rem(xi, 2).astype(F32)
    start = ALPHA * (pair[0] + odd * (pair[1] - pair[0]))
    total = plane_sum(zo, start + sbuf[zo, xi].astype(F32))
    if outer > 1:
        block_wait(zrecv.at[pl.ds(0, outer - 1)], s_send, s_line).wait_recv()
    for p in others:
        total = total + zrecv[p].astype(F32)
    center = row_sum(total) / width
    shifted = total - center
    spread = row_sum(jnp.square(shifted)) / width
    gain = out_gain[...].astype(F32).reshape(1, width)
    out[...] = (shifted * lax.rsqrt(spread + EPS) * gain).astype(BF16)

    def sent(ref, sem):
        block_wait(ref, sem, s_line).wait_send()

    sent(heads_all.at[pl.ds(0, n - 1)], h_send)
    sent(rows_all.at[pl.ds(0, n - 1)], r_send)
    sent(rbuf.at[zo, pl.ds(0, inner - 1)], s_send)

    @pl.when(core == 1)
    def _():
        for p in others:
            sent(rbuf.at[p, pl.ds(0, inner - 1)], s_send)
            sent(zrecv.at[pl.ds(0, 2)], s_send)

    @pl.when(core == 0)
    def _():
        for p in others:
            sent(rbuf.at[p], s_send)

    for c in w_copies:
        c.wait_send()


def on_device(
    n,
    residual,
    query_latent,
    query_rotary,
    latent_new,
    rotary_new,
    latent_cache,
    rotary_cache,
    lengths,
    value_up,
    out_proj,
    attn_gain,
    mix_gate,
    dense_w_gate,
    dense_w_up,
    dense_w_down,
    expert_ids,
    expert_scores,
    expert_gate,
    expert_up,
    expert_down,
    out_gain,
):
    seqs, width = residual.shape
    heads = query_latent.shape[1]
    vu = value_up.transpose(1, 2, 0).reshape(-1, value_up.shape[0])
    rotary_turned = rotary_cache.transpose(0, 2, 1)
    extra = -(-2 * n // 128) * 128
    inner = inner_size(n)
    outer = n // inner
    most = max(1, 128 // (inner * seqs))
    groups = [1] * min(outer, 2)
    while sum(groups) < outer:
        groups.append(min(most, outer - sum(groups)))
    top = max(groups) * inner * seqs
    hbm = pl.BlockSpec(memory_space=pl.ANY)
    dma = pltpu.SemaphoreType.DMA
    block = (outer, inner, seqs, width)
    half_fe = expert_gate.shape[-1]
    fd = dense_w_gate.shape[-1]
    return pl.pallas_call(
        functools.partial(kernel, n, tuple(groups)),
        out_shape=pltpu.VMEM((seqs, width), BF16),
        in_specs=[hbm] * 21,
        out_specs=pl.BlockSpec(memory_space=VMEM),
        scratch_shapes=[
            pltpu.SMEM(lengths.shape, jnp.int32),
            VMEM(query_rotary.shape, BF16),
            VMEM(rotary_new.shape, BF16),
            VMEM(query_latent.shape, BF16),
            VMEM(latent_new.shape, BF16),
            VMEM(rotary_turned.shape, BF16),
            VMEM(latent_cache.shape, BF16),
            VMEM(expert_ids.shape, jnp.int32),
            VMEM(expert_scores.shape, F32),
            VMEM(vu.shape, BF16),
            VMEM(out_proj.shape, BF16),
            VMEM(attn_gain.shape, BF16),
            VMEM(mix_gate.shape, BF16),
            VMEM((2,) + expert_gate.shape[1:], BF16),
            VMEM((2,) + expert_up.shape[1:], BF16),
            VMEM((2 * half_fe + fd, width), BF16),
            VMEM(dense_w_gate.shape, BF16),
            VMEM(dense_w_up.shape, BF16),
            VMEM(out_gain.shape, BF16),
            VMEM((seqs * heads, latent_cache.shape[-1]), F32),
            VMEM((n, seqs, width + extra), BF16),
            VMEM((n, seqs, vu.shape[0]), BF16),
            VMEM((top, width), F32),
            VMEM((top, width), BF16),
            VMEM((inner * seqs, width), BF16),
            VMEM((top, 2 * half_fe + fd), BF16),
            VMEM(block, BF16),
            VMEM(block, BF16),
            VMEM((outer, seqs, width), BF16),
            VMEM((outer, seqs, width), BF16),
            dma((18,)),
            dma,
            dma((3,)),
            dma((3,)),
            dma,
            dma((outer,)),
            dma((outer,)),
            dma,
            dma((outer,)),
            dma,
            dma((outer,)),
            dma,
            pltpu.SemaphoreType.REGULAR,
            VMEM(block, BF16),
            VMEM((outer, seqs, width), BF16),
            dma((outer,)),
        ],
        compiler_params=pltpu.CompilerParams(
            collective_id=0, has_side_effects=True, vmem_limit_bytes=60 * 1024 * 1024
        ),
    )(
        lengths,
        query_rotary,
        rotary_new,
        query_latent,
        latent_new,
        rotary_turned,
        latent_cache,
        residual,
        expert_ids,
        expert_scores,
        vu,
        out_proj,
        attn_gain,
        mix_gate,
        expert_gate,
        expert_up,
        expert_down,
        dense_w_gate,
        dense_w_up,
        dense_w_down,
        out_gain,
    )


def solution(mesh):
    rows = P(("ep", "tp"), None)
    rows3 = P(("ep", "tp"), None, None)
    return jax.shard_map(
        functools.partial(on_device, mesh.shape["ep"]),
        mesh=mesh,
        in_specs=(
            rows,
            rows3,
            rows3,
            rows,
            rows,
            rows3,
            rows3,
            P(("ep", "tp")),
            P(),
            P(),
            P(),
            P(),
            P(None, "ep"),
            P(None, "ep"),
            P("ep", None),
            rows,
            rows,
            P("ep", None, "tp"),
            P("ep", None, "tp"),
            P("ep", "tp", None),
            P(),
        ),
        out_specs=rows,
        check_vma=False,
    )
```
